256 devices in a mesh: kv: 64 (over z, y, core), tp: 4 (over x).
Axes of the slice: x: 4, y: 4, z: 8, core: 2. Of those that a mesh axis runs over, the one named last changes fastest.
Arguments:
- x_piece: bfloat16 [1024, 2048], P('kv'), may hold values from -6 to 6
- x_decode: bfloat16 [64, 2048], P('kv'), may hold values from -6 to 6
- norm_gain: float32 [2048], replicated, may hold values from 0.1 to 1.9
- w_query: bfloat16 [2048, 1024], P(None, 'tp'), may hold values from -0.1875 to 0.1875
- w_key: bfloat16 [2048, 1024], P(None, 'tp'), may hold values from -0.1875 to 0.1875
- w_value: bfloat16 [2048, 1024], P(None, 'tp'), may hold values from -0.125 to 0.125
- w_out: bfloat16 [1024, 2048], P(None, 'tp'), may hold values from -0.1875 to 0.1875
- head_gain: float32 [128], replicated, may hold values from 0.1 to 1.9
- lambdas: float32 [8], P('tp'), may hold values from 0.3 to 0.8
- piece_keys: bfloat16 [32768, 8, 128], P('kv', 'tp'), may hold values from -300 to 300
- piece_values: bfloat16 [32768, 8, 128], P('kv', 'tp'), may hold values from -6 to 6
- cache_keys: bfloat16 [64, 2048, 8, 128], P('kv', None, 'tp'), may hold values from -300 to 300
- cache_values: bfloat16 [64, 2048, 8, 128], P('kv', None, 'tp'), may hold values from -6 to 6
- cache_lengths: int32 [64], P('kv'), may hold values from 1 to 2048, as said below
Outputs:
- piece_out: bfloat16 [1024, 2048], P('kv', 'tp')
- decode_out: bfloat16 [64, 2048], P('kv', 'tp')
The draws below stay inside these ranges and needn't reach their ends.
Inputs may be any that keep to these rules, and one draw needn't show every extreme that they name: `cache_lengths`: some sequence has exactly 2048 filled slots.
All inputs are finite; a program needn't handle non-finite values.
Results may differ from the reference program's by a relative error of at most 0.013.
The reference program's roundings to bfloat16 on the way count: a program that leaves them out, or rounds other values in their place, can miss the bound.
Values may be sent and summed in bfloat16 or wider, within the bound.
No kernel may reach another device: no remote copies, remote signals or barrier semaphores. Data moves between devices by JAX's collectives and lax.ppermute only.
A program may use at most 64 MiB of HBM per device.

```python
import jax
import jax.numpy as jnp
from jax import lax

D = 2048
HEADS = 8
DK = 64
DV = 128
DEC_LEN = 2048
PIECE = 1024
PAST = 32768
DEC = 64


def drawn_keys(key, shape):
    base = jax.random.normal(jax.random.fold_in(key, 11), shape, jnp.float32) * 1.32
    return jnp.clip(base, -300.0, 300.0).astype(jnp.bfloat16)


def draw_piece_keys(key, part):
    return drawn_keys(jax.random.fold_in(key, 21), (PAST, HEADS, 2 * DK))


def draw_cache_keys(key, part):
    return drawn_keys(jax.random.fold_in(key, 22), (DEC, DEC_LEN, HEADS, 2 * DK))


def draw_cache_lengths(key, part):
    first = jax.random.randint(jax.random.fold_in(key, 31), (DEC,), 1, DEC_LEN + 1)
    second = jax.random.randint(jax.random.fold_in(key, 32), (DEC,), 1, DEC_LEN + 1)
    lengths = jnp.minimum(first, second)
    longest = jax.random.randint(jax.random.fold_in(key, 33), (), 0, DEC)
    return lengths.at[longest].set(DEC_LEN).astype(jnp.int32)


def shard_levels(key, shape, pieces, low, largest):
    factor_of = 1.0
    for dim, blocks in pieces:
        draws = jax.random.uniform(jax.random.fold_in(jax.random.fold_in(key, 6), dim), (blocks,), jnp.float32, low / len(pieces), largest / len(pieces))
        factor_of = factor_of * jnp.repeat(jnp.exp(draws), shape[dim] // blocks).reshape((-1,) + (1,) * (len(shape) - 1 - dim))
    return factor_of


def normal_values(own_key, dims, width, limit, pieces=(), held_as=jnp.bfloat16):
    factor_of = shard_levels(own_key, dims, pieces, -0.22, 0.18) if pieces else 1.0
    entries = jax.random.normal(own_key, dims, jnp.float32) * width * factor_of
    return jnp.minimum(jnp.maximum(entries, -limit), limit).astype(held_as)


def setup_inputs(seed: int = 0) -> dict:
    splits = jax.random.split(jax.random.key(seed), 15)
    return {
        "x_piece": normal_values(splits[0], (PIECE, D), 1.0, 6.0, ((0, 64),)),
        "x_decode": normal_values(splits[1], (DEC, D), 1.0, 6.0, ((0, 64),)),
        "norm_gain": jnp.clip(1.0 + 0.18 * jax.random.normal(splits[2], (D,), jnp.float32), 0.1, 1.9),
        "w_query": normal_values(splits[3], (D, HEADS * 2 * DK), (4 * D // 7) ** -0.5, 0.1875, ((1, 4),)),
        "w_key": normal_values(splits[4], (D, HEADS * 2 * DK), (4 * D // 7) ** -0.5, 0.1875, ((1, 4),)),
        "w_value": normal_values(splits[5], (D, HEADS * DV), D ** -0.5, 0.125, ((1, 4),)),
        "w_out": normal_values(splits[6], (HEADS * DV, D), (HEADS * DV) ** -0.5, 0.1875, ((1, 4),)),
        "head_gain": jnp.clip(1.0 + 0.18 * jax.random.normal(splits[7], (DV,), jnp.float32), 0.1, 1.9),
        "lambdas": jnp.clip(0.3 + 0.5 * jax.random.uniform(splits[8], (HEADS,), jnp.float32) ** shard_levels(splits[8], (HEADS,), ((0, 4),), -0.2, 0.2), 0.3, 0.8),
        "piece_keys": draw_piece_keys(jax.random.fold_in(splits[14], 71), 0),
        "piece_values": normal_values(splits[10], (PAST, HEADS, DV), 1.0, 6.0, ((0, 64), (1, 4))),
        "cache_keys": draw_cache_keys(jax.random.fold_in(splits[14], 71), 0),
        "cache_values": normal_values(splits[12], (DEC, DEC_LEN, HEADS, DV), 1.0, 6.0, ((0, 64), (2, 4))),
        "cache_lengths": draw_cache_lengths(jax.random.fold_in(splits[14], 71), 0),
    }


EPS = 1e-06

def project_rows(rows, norm_gain, w_query, w_key, w_value):
    values32 = rows.astype(jnp.float32)
    normed = (values32 * lax.rsqrt(lax.optimization_barrier(jnp.mean(values32 * values32, axis=-1, keepdims=True)) + EPS) * norm_gain).astype(jnp.bfloat16)
    count = rows.shape[0]
    queries = jnp.dot(normed, w_query, preferred_element_type=jnp.float32).astype(jnp.bfloat16).reshape(count, HEADS, 2 * DK)
    new_keys = jnp.dot(normed, w_key, preferred_element_type=jnp.float32).astype(jnp.bfloat16).reshape(count, HEADS, 2 * DK)
    new_values = jnp.dot(normed, w_value, preferred_element_type=jnp.float32).astype(jnp.bfloat16).reshape(count, HEADS, DV)
    return (queries, new_keys, new_values)

def head_norm(attended, head_gain):
    return (attended * lax.rsqrt(lax.optimization_barrier(jnp.mean(attended * attended, axis=-1, keepdims=True)) + EPS) * head_gain).astype(jnp.bfloat16)

def reference(x_piece, x_decode, norm_gain, w_query, w_key, w_value, w_out, head_gain, lambdas, piece_keys, piece_values, cache_keys, cache_values, cache_lengths):
    score_scale = 1.0 / DK ** 0.5
    piece_q, piece_k, piece_v = project_rows(x_piece, norm_gain, w_query, w_key, w_value)
    dec_q, dec_k, dec_v = project_rows(x_decode, norm_gain, w_query, w_key, w_value)
    keys_all = jnp.concatenate([piece_keys, piece_k], axis=0).transpose(1, 0, 2)
    values_all = jnp.concatenate([piece_values, piece_v], axis=0).transpose(1, 0, 2)
    key_index = jnp.arange(PAST + PIECE, dtype=jnp.int32)
    block_rows = 512 if PIECE % 512 == 0 else PIECE
    nblocks = PIECE // block_rows

    def one_head(inputs):
        head_q, head_k, head_v, weight_two = inputs
        blocks = head_q.reshape(nblocks, block_rows, 2 * DK)

        def one_block(binputs):
            query_block, block_start = binputs
            query_pos = block_start + jnp.arange(block_rows, dtype=jnp.int32)
            allowed = (key_index[None, :] < PAST) | (key_index[None, :] - PAST <= query_pos[:, None])
            results = []
            for which_map in range(2):
                lower = which_map * DK
                scores = jnp.dot(query_block[:, lower:lower + DK], head_k[:, lower:lower + DK].T, preferred_element_type=jnp.float32) * score_scale
                scores = jnp.where(allowed, scores, -jnp.inf)
                row_max = lax.optimization_barrier(jnp.max(scores, axis=-1, keepdims=True))
                weights = jnp.exp(scores - row_max)
                totals = lax.optimization_barrier(jnp.sum(weights, axis=-1, keepdims=True))
                mixed = jnp.dot(weights.astype(jnp.bfloat16), head_v, preferred_element_type=jnp.float32)
                results.append(mixed / totals)
            return results[0] - weight_two * results[1]
        starts = jnp.arange(nblocks, dtype=jnp.int32) * block_rows
        return lax.map(one_block, (blocks, starts)).reshape(PIECE, DV)
    piece_att = lax.map(one_head, (piece_q.transpose(1, 0, 2), keys_all, values_all, lambdas))
    piece_att = piece_att.transpose(1, 0, 2)
    slot_index = jnp.arange(DEC_LEN + 1, dtype=jnp.int32)

    def one_sequence(inputs):
        seq_q, seq_k, seq_v, own_k, own_v, length = inputs
        keys = jnp.concatenate([seq_k, own_k[None]], axis=0).astype(jnp.float32)
        values = jnp.concatenate([seq_v, own_v[None]], axis=0).astype(jnp.float32)
        allowed = (slot_index < length) | (slot_index == DEC_LEN)
        query32 = seq_q.astype(jnp.float32)
        results = []
        for which_map in range(2):
            lower = which_map * DK
            scores = jnp.einsum('hd,khd->hk', query32[:, lower:lower + DK], keys[:, :, lower:lower + DK]) * score_scale
            scores = jnp.where(allowed[None, :], scores, -jnp.inf)
            row_max = lax.optimization_barrier(jnp.max(scores, axis=-1, keepdims=True))
            weights = jnp.exp(scores - row_max)
            totals = lax.optimization_barrier(jnp.sum(weights, axis=-1, keepdims=True))
            mixed = jnp.einsum('hk,khd->hd', weights.astype(jnp.bfloat16).astype(jnp.float32), values)
            results.append(mixed / totals)
        return results[0] - lambdas[:, None] * results[1]
    dec_att = lax.map(one_sequence, (dec_q, cache_keys, cache_values, dec_k, dec_v, cache_lengths))
    piece_heads = head_norm(piece_att, head_gain).reshape(PIECE, HEADS * DV)
    dec_heads = head_norm(dec_att, head_gain).reshape(DEC, HEADS * DV)
    piece_out = jnp.dot(piece_heads, w_out, preferred_element_type=jnp.float32).astype(jnp.bfloat16)
    decode_out = jnp.dot(dec_heads, w_out, preferred_element_type=jnp.float32).astype(jnp.bfloat16)
    return (piece_out, decode_out)
```

```python
import math

import jax
import jax.numpy as jnp
from jax import lax
from jax.experimental import pallas as pl
from jax.experimental.pallas import tpu as pltpu
from jax.sharding import PartitionSpec as P

EPS = 1e-06
SHARE = 2
NEG = -jnp.inf
F32 = jnp.float32
BF16 = jnp.bfloat16
MIB = 1024 * 1024


def nt_dot(a, b):
    return lax.dot_general(a, b, (((1,), (1,)), ((), ())), preferred_element_type=F32)


def nn_dot(a, b):
    return lax.dot_general(a, b, (((1,), (0,)), ((), ())), preferred_element_type=F32)


def lane_iota(shape):
    return lax.broadcasted_iota(jnp.int32, shape, len(shape) - 1)


def rms(rows, gain):
    return rows * lax.rsqrt(jnp.mean(rows * rows, axis=-1, keepdims=True) + EPS) * gain


def vmem(count):
    return [pl.BlockSpec(memory_space=pltpu.VMEM)] * count


def prep_body(keys, values, out, wide):
    slots = keys.shape[0] // 2
    for index, source in enumerate((keys, values)):
        wide[index] = source[...].astype(F32)
        for head in range(2):
            out[2 * index + head] = wide[index, pl.ds(head, slots, stride=2), :].astype(BF16)


def prep(keys, values):
    rows = keys.shape[0]
    return pl.pallas_call(
        prep_body,
        out_shape=jax.ShapeDtypeStruct((4, rows // 2, 128), BF16),
        in_specs=vmem(2),
        out_specs=vmem(1)[0],
        scratch_shapes=[pltpu.VMEM((2, rows, 128), F32)],
        compiler_params=pltpu.CompilerParams(vmem_limit_bytes=8 * MIB),
        cost_estimate=pl.CostEstimate(flops=10**8, bytes_accessed=MIB, transcendentals=0),
        name="prep",
    )(keys, values)


def query_body(x, x_dec, gain, w, out, out_dec, normed):
    rows = x.shape[0]
    normed[:rows] = rms(x[...].astype(F32), gain[...]).astype(BF16)
    normed[rows:] = jnp.broadcast_to(
        rms(x_dec[...].astype(F32), gain[...]).astype(BF16), (16, x.shape[1])
    )
    result = nn_dot(normed[...], w[...]).astype(BF16)
    for member in range(out.shape[0]):
        out[member] = result[:rows]
    out_dec[...] = result[rows : rows + 1]


def query_rows(x, x_dec, gain, w, members):
    rows, width = x.shape
    return pl.pallas_call(
        query_body,
        out_shape=(
            jax.ShapeDtypeStruct((members, rows, w.shape[1]), BF16),
            jax.ShapeDtypeStruct((1, w.shape[1]), BF16),
        ),
        in_specs=vmem(4),
        out_specs=tuple(vmem(2)),
        scratch_shapes=[pltpu.VMEM((rows + 16, width), BF16)],
        compiler_params=pltpu.CompilerParams(vmem_limit_bytes=8 * MIB),
        cost_estimate=pl.CostEstimate(flops=10**8, bytes_accessed=MIB, transcendentals=0),
        name="query_rows",
    )(x, x_dec, gain, w)


def decode_body(count, *refs):
    xs = refs[:count]
    (x_dec, gain, w_key, w_value, q_dec, keys, values, length, lambdas, head_gain) = refs[
        count : count + 10
    ]
    k_out, v_out, head_out, normed = refs[count + 10 :]
    rows = xs[0].shape[0]
    for slot, x in enumerate(xs):
        normed[slot * rows : (slot + 1) * rows] = rms(x[...].astype(F32), gain[...]).astype(BF16)
    total = rows * count
    normed[total:] = jnp.broadcast_to(
        rms(x_dec[...].astype(F32), gain[...]).astype(BF16), (16, x_dec.shape[1])
    )
    new_keys = nn_dot(normed[...], w_key[...]).astype(BF16)
    new_values = nn_dot(normed[...], w_value[...]).astype(BF16)
    k_out[...] = new_keys[:total]
    v_out[...] = new_values[:total]

    row = lax.broadcasted_iota(jnp.int32, (8, 128), 0)
    lane = lane_iota((8, 128))
    second = (row // 2) % 2 == 1

    def per_head(line):
        line = line.astype(F32)
        return jnp.where(
            second,
            jnp.broadcast_to(line[:, 128:], (8, 128)),
            jnp.broadcast_to(line[:, :128], (8, 128)),
        )

    half = lane // 64 == row % 2
    queries = jnp.where(half, per_head(q_dec[...]), 0.0)
    own_keys = per_head(new_keys[total : total + 1])
    own_values = per_head(new_values[total : total + 1])
    scale = 0.125 * math.log2(math.e)
    scores = nt_dot(queries.astype(BF16), keys[...])
    width = keys.shape[0]
    column = lane_iota((8, width))
    wide_row = lax.broadcasted_iota(jnp.int32, (8, width), 0)
    allowed = (column % 2 == (wide_row // 2) % 2) & (column // 2 < length[0])
    scores = jnp.where(allowed, scores, NEG)
    own_score = jnp.sum(queries * own_keys, axis=-1, keepdims=True)
    row_max = jnp.maximum(jnp.max(scores, axis=-1, keepdims=True), own_score)
    weights = jnp.exp2((scores - row_max) * scale)
    own_weight = jnp.exp2((own_score - row_max) * scale)
    totals = jnp.sum(weights, axis=-1, keepdims=True) + own_weight
    mixed = nn_dot(weights.astype(BF16), values[...])
    mixed = (mixed + own_weight.astype(BF16).astype(F32) * own_values) / totals
    for head in range(2):
        attended = mixed[2 * head : 2 * head + 1] - lambdas[head] * mixed[2 * head + 1 : 2 * head + 2]
        head_out[:, head * 128 : (head + 1) * 128] = rms(attended, head_gain[...]).astype(BF16)


def decode(xs, x_dec, gain, w_key, w_value, q_dec, keys, values, length, lambdas, head_gain):
    count = len(xs)
    rows, width = xs[0].shape
    smem = pl.BlockSpec(memory_space=pltpu.SMEM)
    return pl.pallas_call(
        lambda *refs: decode_body(count, *refs),
        out_shape=(
            jax.ShapeDtypeStruct((count * rows, 256), BF16),
            jax.ShapeDtypeStruct((count * rows, 256), BF16),
            jax.ShapeDtypeStruct((1, 256), BF16),
        ),
        in_specs=vmem(count + 7) + [smem, smem] + vmem(1),
        out_specs=tuple(vmem(3)),
        scratch_shapes=[pltpu.VMEM((count * rows + 16, width), BF16)],
        compiler_params=pltpu.CompilerParams(vmem_limit_bytes=16 * MIB),
        cost_estimate=pl.CostEstimate(flops=2 * 10**9, bytes_accessed=4 * MIB, transcendentals=0),
        name="decode",
    )(*xs, x_dec, gain, w_key, w_value, q_dec, keys, values, length, lambdas, head_gain)


def attend_body(count, *refs):
    device, queries = refs[:2]
    pools = refs[2 : 2 + count]
    k_new, v_new, out = refs[2 + count :]
    rows = queries.shape[0]
    fresh = k_new.shape[0]
    each = fresh // count
    scale = 0.125 * math.log2(math.e)
    me = device[0]
    block = min(256, rows)
    key_lane = lane_iota((block, fresh))
    key_pos = each * jnp.bitwise_xor(key_lane // each, me) + key_lane % each
    row = lax.broadcasted_iota(jnp.int32, (block, fresh), 0)
    lane = lane_iota((block, 128))
    for start in range(0, rows, block):
        at = row + start
        row_pos = each * (count * (at // each) + lax.rem(me, count)) + at % each
        allowed = key_pos <= row_pos
        stats = jnp.zeros((block, 128), F32)
        for head in range(2):
            cols = slice(head * 128, (head + 1) * 128)
            q = queries[start : start + block, cols].astype(F32)
            for which in range(2):
                combo = 2 * head + which
                kept = (lane < 64) if which == 0 else (lane >= 64)
                masked = jnp.where(kept, q, 0.0).astype(BF16)
                scores = [nt_dot(masked, pool[head]) for pool in pools]
                last = jnp.where(allowed, nt_dot(masked, k_new[:, cols]), NEG)
                row_max = jnp.max(last, axis=-1, keepdims=True)
                for s in scores:
                    row_max = jnp.maximum(row_max, jnp.max(s, axis=-1, keepdims=True))
                weights = jnp.exp2((last - row_max) * scale)
                total = jnp.sum(weights, axis=-1, keepdims=True)
                mixed = nn_dot(weights.astype(BF16), v_new[:, cols])
                for s, pool in zip(scores, pools):
                    weights = jnp.exp2((s - row_max) * scale)
                    total = total + jnp.sum(weights, axis=-1, keepdims=True)
                    mixed = mixed + nn_dot(weights.astype(BF16), pool[2 + head])
                mixed = mixed / total
                out[start : start + block, combo * 128 : (combo + 1) * 128] = mixed.astype(BF16)
                for base, stat in ((0, row_max), (4, total)):
                    for part in range(3):
                        piece = stat.astype(BF16).astype(F32)
                        stats = jnp.where(lane == 8 * part + base + combo, piece, stats)
                        stat = stat - piece
        out[start : start + block, 512:640] = stats.astype(BF16)


def attend(device, queries, pools, k_new, v_new):
    count = len(pools)
    rows = queries.shape[0]
    keys = count * pools[0].shape[1] + k_new.shape[0]
    return pl.pallas_call(
        lambda *refs: attend_body(count, *refs),
        out_shape=jax.ShapeDtypeStruct((rows, 640), BF16),
        in_specs=[pl.BlockSpec(memory_space=pltpu.SMEM)] + vmem(count + 3),
        out_specs=vmem(1)[0],
        compiler_params=pltpu.CompilerParams(vmem_limit_bytes=32 * MIB),
        cost_estimate=pl.CostEstimate(
            flops=4 * rows * keys * 512, bytes_accessed=2 * MIB, transcendentals=4 * rows * keys
        ),
        name="attend",
    )(device, queries, *pools, k_new, v_new)


def combine_body(parts, dec_out, lambdas, head_gain, out):
    scale = 0.125 * math.log2(math.e)
    members = parts.shape[0]
    rows = parts.shape[1]

    def whole(member):
        pieces = parts[member, :, 512:640].astype(F32)
        return pieces + pltpu.roll(pieces, 120, 1) + pltpu.roll(pieces, 112, 1)

    stats = [whole(member) for member in range(members)]
    top = stats[0]
    for s in stats[1:]:
        top = jnp.maximum(top, s)
    shares = [jnp.exp2((s - top) * scale) * pltpu.roll(s, 124, 1) for s in stats]
    total = shares[0]
    for s in shares[1:]:
        total = total + s
    sums = []
    for combo in range(4):
        acc = jnp.zeros((rows, 128), F32)
        for member in range(members):
            acc = acc + shares[member][:, combo : combo + 1] * parts[
                member, :, combo * 128 : (combo + 1) * 128
            ].astype(F32)
        sums.append(acc / total[:, combo : combo + 1])
    heads = []
    for head in range(2):
        attended = sums[2 * head] - lambdas[head] * sums[2 * head + 1]
        heads.append(rms(attended, head_gain[...]).astype(BF16))
    for copy in range(out.shape[0]):
        for head in range(2):
            out[copy, :rows, head * 128 : (head + 1) * 128] = heads[head]
        out[copy, rows:, :] = jnp.broadcast_to(dec_out[...], (out.shape[1] - rows, 256))


def combine(parts, dec_out, lambdas, head_gain, copies):
    return pl.pallas_call(
        combine_body,
        out_shape=jax.ShapeDtypeStruct((copies, parts.shape[1] + 8, 256), BF16),
        in_specs=vmem(2) + [pl.BlockSpec(memory_space=pltpu.SMEM)] + vmem(1),
        out_specs=vmem(1)[0],
        compiler_params=pltpu.CompilerParams(vmem_limit_bytes=16 * MIB),
        cost_estimate=pl.CostEstimate(flops=10**8, bytes_accessed=MIB, transcendentals=0),
        name="combine",
    )(parts, dec_out, lambdas, head_gain)


def out_body(heads, w, piece, dec):
    rows = piece.shape[0]
    acc = nn_dot(heads[0], w[:256])
    for copy in range(1, heads.shape[0]):
        acc = acc + nn_dot(heads[copy], w[copy * 256 : (copy + 1) * 256])
    piece[...] = acc[:rows].astype(BF16)
    dec[...] = acc[rows : rows + 1].astype(BF16)


def out_rows(heads, w, rows):
    return pl.pallas_call(
        out_body,
        out_shape=(
            jax.ShapeDtypeStruct((rows, w.shape[1]), BF16),
            jax.ShapeDtypeStruct((1, w.shape[1]), BF16),
        ),
        in_specs=vmem(2),
        out_specs=tuple(vmem(2)),
        compiler_params=pltpu.CompilerParams(vmem_limit_bytes=8 * MIB),
        cost_estimate=pl.CostEstimate(flops=10**8, bytes_accessed=MIB, transcendentals=0),
        name="out_rows",
    )(heads, w)


def shards(
    x_piece,
    x_decode,
    norm_gain,
    w_query,
    w_key,
    w_value,
    w_out,
    head_gain,
    lambdas,
    piece_keys,
    piece_values,
    cache_keys,
    cache_values,
    cache_lengths,
):
    kv_count = lax.axis_size("kv")
    tp_count = lax.axis_size("tp")
    members = kv_count // SHARE
    rows = x_piece.shape[0]
    groups = [[SHARE * m + e for m in range(members)] for e in range(SHARE)]
    gain = norm_gain.reshape(1, -1)
    head_gain = head_gain.reshape(1, -1)
    me = lax.axis_index("kv").reshape(1)

    def swap(array, bit):
        return lax.ppermute(array, "kv", [(i, i ^ bit) for i in range(kv_count)])

    pools = [prep(piece_keys.reshape(-1, 128), piece_values.reshape(-1, 128))]
    xs = [x_piece]
    bit = SHARE // 2
    while bit:
        pools, xs = (
            [p for pool in pools for p in (pool, swap(pool, bit))],
            [p for x in xs for p in (x, swap(x, bit))],
        )
        bit //= 2

    sent, q_dec = query_rows(x_piece, x_decode, gain, w_query, members)
    got = lax.all_to_all(sent, "kv", 0, 0, tiled=True, axis_index_groups=groups)
    k_new, v_new, dec_out = decode(
        xs,
        x_decode,
        gain,
        w_key,
        w_value,
        q_dec,
        cache_keys.reshape(-1, 128),
        cache_values.reshape(-1, 128),
        cache_lengths,
        lambdas,
        head_gain,
    )
    parts = attend(me, got.reshape(members * rows, 256), pools, k_new, v_new)
    parts = lax.all_to_all(
        parts.reshape(members, rows, 640), "kv", 0, 0, tiled=True, axis_index_groups=groups
    )
    heads = combine(parts, dec_out, lambdas, head_gain, tp_count)
    heads = lax.all_to_all(heads, "tp", 0, 0, tiled=True)
    return out_rows(heads, w_out, rows)


def solution(mesh):
    placed = (
        P("kv", None),
        P("kv", None),
        P(),
        P(None, "tp"),
        P(None, "tp"),
        P(None, "tp"),
        P(None, "tp"),
        P(),
        P("tp"),
        P("kv", "tp", None),
        P("kv", "tp", None),
        P("kv", None, "tp", None),
        P("kv", None, "tp", None),
        P("kv"),
    )
    return jax.shard_map(
        shards,
        mesh=mesh,
        in_specs=placed,
        out_specs=(P("kv", "tp"), P("kv", "tp")),
        check_vma=False,
    )
```

```python
import math

import jax
import jax.numpy as jnp
from jax import lax
from jax.experimental import pallas as pl
from jax.experimental.pallas import tpu as pltpu
from jax.sharding import PartitionSpec as P

EPS = 1e-06
SHARE = 4
NEG = -jnp.inf
F32 = jnp.float32
BF16 = jnp.bfloat16
MIB = 1024 * 1024


def nt_dot(a, b):
    return lax.dot_general(a, b, (((1,), (1,)), ((), ())), preferred_element_type=F32)


def nn_dot(a, b):
    return lax.dot_general(a, b, (((1,), (0,)), ((), ())), preferred_element_type=F32)


def lane_iota(shape):
    return lax.broadcasted_iota(jnp.int32, shape, len(shape) - 1)


def rms(rows, gain):
    return rows * lax.rsqrt(jnp.mean(rows * rows, axis=-1, keepdims=True) + EPS) * gain


def vmem(count):
    return [pl.BlockSpec(memory_space=pltpu.VMEM)] * count


HBM = pl.BlockSpec(memory_space=pltpu.HBM)


def fetch(pairs, sems):
    copies = [pltpu.make_async_copy(a, b, sems.at[i]) for i, (a, b) in enumerate(pairs)]
    for copy in copies:
        copy.start()
    return copies


def opening_body(
    keys, values, x, x_dec, gain, w, pool, out, out_dec, kv, xs, xd, g, wq, wide, normed, sems
):
    copies = fetch(
        (
            (x, xs),
            (x_dec, xd),
            (gain, g),
            (keys, kv.at[0]),
            (values, kv.at[1]),
            (w, wq),
        ),
        sems,
    )
    slots = keys.shape[0] // 2
    rows = x.shape[0]
    for copy in copies[:3]:
        copy.wait()
    normed[:rows] = rms(xs[...].astype(F32), g[...]).astype(BF16)
    normed[rows:] = jnp.broadcast_to(
        rms(xd[...].astype(F32), g[...]).astype(BF16), (16, x.shape[1])
    )
    for tile in range(x.shape[1] // 128):
        at = slots + rows * (tile // 4)
        pool[tile % 4, at : at + rows, :] = xs[:, tile * 128 : (tile + 1) * 128]
    for index in range(2):
        copies[3 + index].wait()
        wide[index] = kv[index].astype(F32)
        for head in range(2):
            pool[2 * index + head, :slots] = wide[index, pl.ds(head, slots, stride=2), :].astype(
                BF16
            )
    copies[5].wait()
    result = nn_dot(normed[...], wq[...]).astype(BF16)
    for member in range(out.shape[0]):
        out[member] = result[:rows]
    out_dec[...] = result[rows : rows + 1]


def opening(keys, values, x, x_dec, gain, w, members):
    rows, width = x.shape
    slots = keys.shape[0] // 2
    return pl.pallas_call(
        opening_body,
        out_shape=(
            jax.ShapeDtypeStruct((4, slots + rows * width // 512, 128), BF16),
            jax.ShapeDtypeStruct((members, rows, w.shape[1]), BF16),
            jax.ShapeDtypeStruct((1, w.shape[1]), BF16),
        ),
        in_specs=[HBM] * 6,
        out_specs=tuple(vmem(3)),
        scratch_shapes=[
            pltpu.VMEM((2, 2 * slots, 128), BF16),
            pltpu.VMEM((rows, width), BF16),
            pltpu.VMEM((1, width), BF16),
            pltpu.VMEM((1, width), F32),
            pltpu.VMEM(w.shape, BF16),
            pltpu.VMEM((2, 2 * slots, 128), F32),
            pltpu.VMEM((rows + 16, width), BF16),
            pltpu.SemaphoreType.DMA((6,)),
        ],
        compiler_params=pltpu.CompilerParams(vmem_limit_bytes=60 * 1024 * 1024),
        cost_estimate=pl.CostEstimate(flops=10**9, bytes_accessed=2 * MIB, transcendentals=0),
        name="opening",
    )(keys, values, x, x_dec, gain, w)


def decode_body(
    x_dec, gain, w_key, w_value, q_dec, keys, values, length, lambdas, head_gain, head_out,
    xd, g, wk, wv, kc, vc, sems
):
    copies = fetch(
        ((x_dec, xd), (gain, g), (w_key, wk), (keys, kc), (w_value, wv), (values, vc)), sems
    )
    for copy in copies[:2]:
        copy.wait()
    normed = jnp.broadcast_to(rms(xd[...].astype(F32), g[...]).astype(BF16), (16, xd.shape[1]))
    copies[2].wait()
    new_keys = nn_dot(normed, wk[...]).astype(BF16)[:1]

    row = lax.broadcasted_iota(jnp.int32, (8, 128), 0)
    lane = lane_iota((8, 128))
    second = (row // 2) % 2 == 1

    def per_head(line):
        line = line.astype(F32)
        return jnp.where(
            second,
            jnp.broadcast_to(line[:, 128:], (8, 128)),
            jnp.broadcast_to(line[:, :128], (8, 128)),
        )

    half = lane // 64 == row % 2
    queries = jnp.where(half, per_head(q_dec[...]), 0.0)
    own_keys = per_head(new_keys)
    scale = 0.125 * math.log2(math.e)
    copies[3].wait()
    scores = nt_dot(queries.astype(BF16), kc[...])
    width = keys.shape[0]
    column = lane_iota((8, width))
    wide_row = lax.broadcasted_iota(jnp.int32, (8, width), 0)
    allowed = (column % 2 == (wide_row // 2) % 2) & (column // 2 < length[0])
    scores = jnp.where(allowed, scores, NEG)
    own_score = jnp.sum(queries * own_keys, axis=-1, keepdims=True)
    row_max = jnp.maximum(jnp.max(scores, axis=-1, keepdims=True), own_score)
    weights = jnp.exp2((scores - row_max) * scale)
    own_weight = jnp.exp2((own_score - row_max) * scale)
    totals = jnp.sum(weights, axis=-1, keepdims=True) + own_weight
    copies[4].wait()
    own_values = per_head(nn_dot(normed, wv[...]).astype(BF16)[:1])
    copies[5].wait()
    mixed = nn_dot(weights.astype(BF16), vc[...])
    mixed = (mixed + own_weight.astype(BF16).astype(F32) * own_values) / totals
    for head in range(2):
        attended = mixed[2 * head : 2 * head + 1] - lambdas[head] * mixed[2 * head + 1 : 2 * head + 2]
        head_out[:, head * 128 : (head + 1) * 128] = rms(attended, head_gain[...]).astype(BF16)


def decode(x_dec, gain, w_key, w_value, q_dec, keys, values, length, lambdas, head_gain):
    smem = pl.BlockSpec(memory_space=pltpu.SMEM)
    return pl.pallas_call(
        decode_body,
        out_shape=jax.ShapeDtypeStruct((1, 256), BF16),
        in_specs=[HBM] * 4 + vmem(1) + [HBM] * 2 + [smem, smem] + vmem(1),
        out_specs=vmem(1)[0],
        scratch_shapes=[
            pltpu.VMEM(x_dec.shape, BF16),
            pltpu.VMEM(gain.shape, F32),
            pltpu.VMEM(w_key.shape, BF16),
            pltpu.VMEM(w_value.shape, BF16),
            pltpu.VMEM(keys.shape, BF16),
            pltpu.VMEM(values.shape, BF16),
            pltpu.SemaphoreType.DMA((6,)),
        ],
        compiler_params=pltpu.CompilerParams(vmem_limit_bytes=60 * 1024 * 1024),
        cost_estimate=pl.CostEstimate(flops=2 * 10**9, bytes_accessed=4 * MIB, transcendentals=0),
        name="decode",
    )(x_dec, gain, w_key, w_value, q_dec, keys, values, length, lambdas, head_gain)


def fresh_body(*refs):
    (gain, w_key, w_value) = refs[:3]
    pools = refs[3:-6]
    (k_out, v_out, wk, wv, normed, sems) = refs[-6:]
    copies = fetch(((w_key, wk), (w_value, wv)), sems)
    rows = k_out.shape[0] // len(pools)
    tiles = gain.shape[1] // 128
    slots = pools[0].shape[1] - rows * tiles // 4
    for slot, pool in enumerate(pools):
        parts = []
        for tile in range(tiles):
            at = slots + rows * (tile // 4)
            parts.append(pool[tile % 4, at : at + rows, :])
        x = jnp.concatenate(parts, axis=1).astype(F32)
        normed[slot * rows : (slot + 1) * rows] = rms(x, gain[...]).astype(BF16)
    copies[0].wait()
    k_out[...] = nn_dot(normed[...], wk[...]).astype(BF16)
    copies[1].wait()
    v_out[...] = nn_dot(normed[...], wv[...]).astype(BF16)


def fresh(gain, w_key, w_value, pools, rows):
    total = rows * len(pools)
    return pl.pallas_call(
        fresh_body,
        out_shape=(jax.ShapeDtypeStruct((total, 256), BF16),) * 2,
        in_specs=vmem(1) + [HBM] * 2 + vmem(len(pools)),
        out_specs=tuple(vmem(2)),
        scratch_shapes=[
            pltpu.VMEM(w_key.shape, BF16),
            pltpu.VMEM(w_value.shape, BF16),
            pltpu.VMEM((total, gain.shape[1]), BF16),
            pltpu.SemaphoreType.DMA((2,)),
        ],
        compiler_params=pltpu.CompilerParams(vmem_limit_bytes=8 * MIB),
        cost_estimate=pl.CostEstimate(flops=10**9, bytes_accessed=2 * MIB, transcendentals=0),
        name="fresh",
    )(gain, w_key, w_value, *pools)


def attend_body(count, slots, *refs):
    device, queries = refs[:2]
    pools = refs[2 : 2 + count]
    k_new, v_new, out = refs[2 + count :]
    rows = queries.shape[0]
    fresh = k_new.shape[0]
    each = fresh // count
    scale = 0.125 * math.log2(math.e)
    me = device[0]
    block = min(256, rows)
    key_lane = lane_iota((block, fresh))
    key_pos = each * jnp.bitwise_xor(key_lane // each, me) + key_lane % each
    row = lax.broadcasted_iota(jnp.int32, (block, fresh), 0)
    lane = lane_iota((block, 128))
    for start in range(0, rows, block):
        at = row + start
        row_pos = each * (count * (at // each) + lax.rem(me, count)) + at % each
        allowed = key_pos <= row_pos
        stats = jnp.zeros((block, 128), F32)
        for head in range(2):
            cols = slice(head * 128, (head + 1) * 128)
            q = queries[start : start + block, cols].astype(F32)
            for which in range(2):
                combo = 2 * head + which
                kept = (lane < 64) if which == 0 else (lane >= 64)
                masked = jnp.where(kept, q, 0.0).astype(BF16)
                scores = [nt_dot(masked, pool[head, :slots]) for pool in pools]
                last = jnp.where(allowed, nt_dot(masked, k_new[:, cols]), NEG)
                row_max = jnp.max(last, axis=-1, keepdims=True)
                for s in scores:
                    row_max = jnp.maximum(row_max, jnp.max(s, axis=-1, keepdims=True))
                weights = jnp.exp2((last - row_max) * scale)
                total = jnp.sum(weights, axis=-1, keepdims=True)
                mixed = nn_dot(weights.astype(BF16), v_new[:, cols])
                for s, pool in zip(scores, pools):
                    weights = jnp.exp2((s - row_max) * scale)
                    total = total + jnp.sum(weights, axis=-1, keepdims=True)
                    mixed = mixed + nn_dot(weights.astype(BF16), pool[2 + head, :slots])
                mixed = mixed / total
                out[start : start + block, combo * 128 : (combo + 1) * 128] = mixed.astype(BF16)
                for base, stat in ((0, row_max), (4, total)):
                    for part in range(3):
                        piece = stat.astype(BF16).astype(F32)
                        stats = jnp.where(lane == 8 * part + base + combo, piece, stats)
                        stat = stat - piece
        out[start : start + block, 512:640] = stats.astype(BF16)


def attend(device, queries, pools, slots, k_new, v_new):
    count = len(pools)
    rows = queries.shape[0]
    keys = count * slots + k_new.shape[0]
    return pl.pallas_call(
        lambda *refs: attend_body(count, slots, *refs),
        out_shape=jax.ShapeDtypeStruct((rows, 640), BF16),
        in_specs=[pl.BlockSpec(memory_space=pltpu.SMEM)] + vmem(count + 3),
        out_specs=vmem(1)[0],
        compiler_params=pltpu.CompilerParams(vmem_limit_bytes=32 * MIB),
        cost_estimate=pl.CostEstimate(
            flops=4 * rows * keys * 512, bytes_accessed=2 * MIB, transcendentals=4 * rows * keys
        ),
        name="attend",
    )(device, queries, *pools, k_new, v_new)


def combine_body(parts, dec_out, lambdas, head_gain, out):
    scale = 0.125 * math.log2(math.e)
    members = parts.shape[0]
    rows = parts.shape[1]

    def whole(member):
        pieces = parts[member, :, 512:640].astype(F32)
        return pieces + pltpu.roll(pieces, 120, 1) + pltpu.roll(pieces, 112, 1)

    stats = [whole(member) for member in range(members)]
    top = stats[0]
    for s in stats[1:]:
        top = jnp.maximum(top, s)
    shares = [jnp.exp2((s - top) * scale) * pltpu.roll(s, 124, 1) for s in stats]
    total = shares[0]
    for s in shares[1:]:
        total = total + s
    sums = []
    for combo in range(4):
        acc = jnp.zeros((rows, 128), F32)
        for member in range(members):
            acc = acc + shares[member][:, combo : combo + 1] * parts[
                member, :, combo * 128 : (combo + 1) * 128
            ].astype(F32)
        sums.append(acc / total[:, combo : combo + 1])
    heads = []
    for head in range(2):
        attended = sums[2 * head] - lambdas[head] * sums[2 * head + 1]
        heads.append(rms(attended, head_gain[...]).astype(BF16))
    for copy in range(out.shape[0]):
        for head in range(2):
            out[copy, :rows, head * 128 : (head + 1) * 128] = heads[head]
        out[copy, rows:, :] = jnp.broadcast_to(dec_out[...], (out.shape[1] - rows, 256))


def combine(parts, dec_out, lambdas, head_gain, copies):
    return pl.pallas_call(
        combine_body,
        out_shape=jax.ShapeDtypeStruct((copies, parts.shape[1] + 8, 256), BF16),
        in_specs=vmem(2) + [pl.BlockSpec(memory_space=pltpu.SMEM)] + vmem(1),
        out_specs=vmem(1)[0],
        compiler_params=pltpu.CompilerParams(vmem_limit_bytes=16 * MIB),
        cost_estimate=pl.CostEstimate(flops=10**8, bytes_accessed=MIB, transcendentals=0),
        name="combine",
    )(parts, dec_out, lambdas, head_gain)


def out_body(heads, w, piece, dec):
    rows = piece.shape[0]
    acc = nn_dot(heads[0], w[:256])
    for copy in range(1, heads.shape[0]):
        acc = acc + nn_dot(heads[copy], w[copy * 256 : (copy + 1) * 256])
    piece[...] = acc[:rows].astype(BF16)
    dec[...] = acc[rows : rows + 1].astype(BF16)


def out_rows(heads, w, rows):
    return pl.pallas_call(
        out_body,
        out_shape=(
            jax.ShapeDtypeStruct((rows, w.shape[1]), BF16),
            jax.ShapeDtypeStruct((1, w.shape[1]), BF16),
        ),
        in_specs=vmem(2),
        out_specs=tuple(vmem(2)),
        compiler_params=pltpu.CompilerParams(vmem_limit_bytes=8 * MIB),
        cost_estimate=pl.CostEstimate(flops=10**8, bytes_accessed=MIB, transcendentals=0),
        name="out_rows",
    )(heads, w)


def layer(
    x_piece,
    x_decode,
    norm_gain,
    w_query,
    w_key,
    w_value,
    w_out,
    head_gain,
    lambdas,
    piece_keys,
    piece_values,
    cache_keys,
    cache_values,
    cache_lengths,
):
    kv_count = lax.axis_size("kv")
    tp_count = lax.axis_size("tp")
    members = kv_count // SHARE
    rows = x_piece.shape[0]
    groups = [[SHARE * m + e for m in range(members)] for e in range(SHARE)]
    gain = norm_gain.reshape(1, -1)
    head_gain = head_gain.reshape(1, -1)
    me = lax.axis_index("kv").reshape(1)

    def swap(array, bit):
        return lax.ppermute(array, "kv", [(i, i ^ bit) for i in range(kv_count)])

    pool, sent, q_dec = opening(
        piece_keys.reshape(-1, 128),
        piece_values.reshape(-1, 128),
        x_piece,
        x_decode,
        gain,
        w_query,
        members,
    )
    pools = [pool]
    bit = SHARE // 2
    while bit:
        swapped = []
        for pool in pools:
            swapped += [pool, swap(pool, bit)]
        pools = swapped
        bit //= 2
    got = lax.all_to_all(sent, "kv", 0, 0, tiled=True, axis_index_groups=groups)
    dec_out = decode(
        x_decode,
        gain,
        w_key,
        w_value,
        q_dec,
        cache_keys.reshape(-1, 128),
        cache_values.reshape(-1, 128),
        cache_lengths,
        lambdas,
        head_gain,
    )
    k_new, v_new = fresh(gain, w_key, w_value, pools, rows)
    slots = piece_keys.shape[0]
    parts = attend(me, got.reshape(members * rows, 256), pools, slots, k_new, v_new)
    parts = lax.all_to_all(
        parts.reshape(members, rows, 640), "kv", 0, 0, tiled=True, axis_index_groups=groups
    )
    heads = combine(parts, dec_out, lambdas, head_gain, tp_count)
    heads = lax.all_to_all(heads, "tp", 0, 0, tiled=True)
    return out_rows(heads, w_out, rows)


def solution(mesh):
    placed = (
        P("kv", None),
        P("kv", None),
        P(),
        P(None, "tp"),
        P(None, "tp"),
        P(None, "tp"),
        P(None, "tp"),
        P(),
        P("tp"),
        P("kv", "tp", None),
        P("kv", "tp", None),
        P("kv", None, "tp", None),
        P("kv", None, "tp", None),
        P("kv"),
    )
    return jax.shard_map(
        layer,
        mesh=mesh,
        in_specs=placed,
        out_specs=(P("kv", "tp"), P("kv", "tp")),
        check_vma=False,
    )
```

```python
import math

import jax
import jax.numpy as jnp
from jax import lax
from jax.experimental import pallas as pl
from jax.experimental.pallas import tpu as pltpu
from jax.sharding import PartitionSpec as P

EPS = 1e-06
SHARE = 4
NEG = -jnp.inf
F32 = jnp.float32
BF16 = jnp.bfloat16
MIB = 1024 * 1024
ATT, FRE, DEC, OPN = 20, 8, 16, 60


def nt_dot(a, b):
    return lax.dot_general(a, b, (((1,), (1,)), ((), ())), preferred_element_type=F32)


def nn_dot(a, b):
    return lax.dot_general(a, b, (((1,), (0,)), ((), ())), preferred_element_type=F32)


def lane_iota(shape):
    return lax.broadcasted_iota(jnp.int32, shape, len(shape) - 1)


def rms(rows, gain):
    return rows * lax.rsqrt(jnp.mean(rows * rows, axis=-1, keepdims=True) + EPS) * gain


def vmem(count):
    return [pl.BlockSpec(memory_space=pltpu.VMEM)] * count


HBM = pl.BlockSpec(memory_space=pltpu.HBM)


def fetch(pairs, sems):
    copies = [pltpu.make_async_copy(a, b, sems.at[i]) for i, (a, b) in enumerate(pairs)]
    for copy in copies:
        copy.start()
    return copies


def opening_body(
    keys, values, x, x_dec, gain, w, pool0, pool1, out, out_dec, kv, xs, xd, g, wq, wide, normed, sems
):
    pools = (pool0, pool1)
    copies = fetch(
        (
            (x, xs),
            (x_dec, xd),
            (gain, g),
            (keys, kv.at[0]),
            (values, kv.at[1]),
            (w, wq),
        ),
        sems,
    )
    slots = keys.shape[0] // 2
    rows = x.shape[0]
    for copy in copies[:3]:
        copy.wait()
    normed[:rows] = rms(xs[...].astype(F32), g[...]).astype(BF16)
    normed[rows:] = jnp.broadcast_to(
        rms(xd[...].astype(F32), g[...]).astype(BF16), (16, x.shape[1])
    )
    for tile in range(x.shape[1] // 128):
        at = slots + rows * (tile // 2)
        for pool in pools:
            pool[tile % 2, at : at + rows, :] = xs[:, tile * 128 : (tile + 1) * 128]
    for index in range(2):
        copies[3 + index].wait()
        wide[index] = kv[index].astype(F32)
        for head in range(2):
            pools[head][index, :slots] = wide[index, pl.ds(head, slots, stride=2), :].astype(BF16)
    copies[5].wait()
    result = nn_dot(normed[...], wq[...]).astype(BF16)
    for member in range(out.shape[0]):
        out[member] = result[:rows]
    out_dec[...] = result[rows : rows + 1]


def opening(keys, values, x, x_dec, gain, w, members):
    rows, width = x.shape
    slots = keys.shape[0] // 2
    return pl.pallas_call(
        opening_body,
        out_shape=(
            jax.ShapeDtypeStruct((2, slots + rows * width // 256, 128), BF16),
            jax.ShapeDtypeStruct((2, slots + rows * width // 256, 128), BF16),
            jax.ShapeDtypeStruct((members, rows, w.shape[1]), BF16),
            jax.ShapeDtypeStruct((1, w.shape[1]), BF16),
        ),
        in_specs=[HBM] * 6,
        out_specs=tuple(vmem(4)),
        scratch_shapes=[
            pltpu.VMEM((2, 2 * slots, 128), BF16),
            pltpu.VMEM((rows, width), BF16),
            pltpu.VMEM((1, width), BF16),
            pltpu.VMEM((1, width), F32),
            pltpu.VMEM(w.shape, BF16),
            pltpu.VMEM((2, 2 * slots, 128), F32),
            pltpu.VMEM((rows + 16, width), BF16),
            pltpu.SemaphoreType.DMA((6,)),
        ],
        compiler_params=pltpu.CompilerParams(vmem_limit_bytes=OPN * MIB),
        cost_estimate=pl.CostEstimate(flops=10**9, bytes_accessed=2 * MIB, transcendentals=0),
        name="opening",
    )(keys, values, x, x_dec, gain, w)


def decode_body(
    x_dec, gain, w_key, w_value, q_dec, keys, values, length, lambdas, head_gain, head_out,
    xd, g, wk, wv, kc, vc, sems
):
    copies = fetch(
        ((x_dec, xd), (gain, g), (w_key, wk), (keys, kc), (w_value, wv), (values, vc)), sems
    )
    for copy in copies[:2]:
        copy.wait()
    normed = jnp.broadcast_to(rms(xd[...].astype(F32), g[...]).astype(BF16), (16, xd.shape[1]))
    copies[2].wait()
    new_keys = nn_dot(normed, wk[...]).astype(BF16)[:1]

    row = lax.broadcasted_iota(jnp.int32, (8, 128), 0)
    lane = lane_iota((8, 128))
    second = (row // 2) % 2 == 1

    def per_head(line):
        line = line.astype(F32)
        return jnp.where(
            second,
            jnp.broadcast_to(line[:, 128:], (8, 128)),
            jnp.broadcast_to(line[:, :128], (8, 128)),
        )

    half = lane // 64 == row % 2
    queries = jnp.where(half, per_head(q_dec[...]), 0.0)
    own_keys = per_head(new_keys)
    scale = 0.125 * math.log2(math.e)
    copies[3].wait()
    scores = nt_dot(queries.astype(BF16), kc[...])
    width = keys.shape[0]
    column = lane_iota((8, width))
    wide_row = lax.broadcasted_iota(jnp.int32, (8, width), 0)
    allowed = (column % 2 == (wide_row // 2) % 2) & (column // 2 < length[0])
    scores = jnp.where(allowed, scores, NEG)
    own_score = jnp.sum(queries * own_keys, axis=-1, keepdims=True)
    row_max = jnp.maximum(jnp.max(scores, axis=-1, keepdims=True), own_score)
    weights = jnp.exp2((scores - row_max) * scale)
    own_weight = jnp.exp2((own_score - row_max) * scale)
    totals = jnp.sum(weights, axis=-1, keepdims=True) + own_weight
    copies[4].wait()
    own_values = per_head(nn_dot(normed, wv[...]).astype(BF16)[:1])
    copies[5].wait()
    mixed = nn_dot(weights.astype(BF16), vc[...])
    mixed = (mixed + own_weight.astype(BF16).astype(F32) * own_values) / totals
    for head in range(2):
        attended = mixed[2 * head : 2 * head + 1] - lambdas[head] * mixed[2 * head + 1 : 2 * head + 2]
        head_out[:, head * 128 : (head + 1) * 128] = rms(attended, head_gain[...]).astype(BF16)


def decode(x_dec, gain, w_key, w_value, q_dec, keys, values, length, lambdas, head_gain):
    smem = pl.BlockSpec(memory_space=pltpu.SMEM)
    return pl.pallas_call(
        decode_body,
        out_shape=jax.ShapeDtypeStruct((1, 256), BF16),
        in_specs=[HBM] * 4 + vmem(1) + [HBM] * 2 + [smem, smem] + vmem(1),
        out_specs=vmem(1)[0],
        scratch_shapes=[
            pltpu.VMEM(x_dec.shape, BF16),
            pltpu.VMEM(gain.shape, F32),
            pltpu.VMEM(w_key.shape, BF16),
            pltpu.VMEM(w_value.shape, BF16),
            pltpu.VMEM(keys.shape, BF16),
            pltpu.VMEM(values.shape, BF16),
            pltpu.SemaphoreType.DMA((6,)),
        ],
        compiler_params=pltpu.CompilerParams(vmem_limit_bytes=DEC * MIB),
        cost_estimate=pl.CostEstimate(flops=2 * 10**9, bytes_accessed=4 * MIB, transcendentals=0),
        name="decode",
    )(x_dec, gain, w_key, w_value, q_dec, keys, values, length, lambdas, head_gain)


def fresh_body(*refs):
    gain, w_key, w_value = refs[:3]
    sources = refs[3:9]
    k_out, v_out, normed = refs[9:]
    rows = k_out.shape[0] // 4
    tiles = gain.shape[1] // 128
    slots = sources[0].shape[1] - rows * tiles // 2
    for index, source in enumerate(sources):
        parts = [
            source[tile % 2, slots + rows * (tile // 2) : slots + rows * (tile // 2 + 1), :]
            for tile in range(tiles)
        ]
        x = jnp.concatenate(parts, axis=1).astype(F32)
        normed[index * rows : (index + 1) * rows] = rms(x, gain[...]).astype(BF16)
    for w, out in ((w_key, k_out), (w_value, v_out)):
        result = nn_dot(normed[...], w[...]).astype(BF16)
        out[:, :128] = result[: 4 * rows, :128]
        out[: 2 * rows, 128:] = result[: 2 * rows, 128:]
        out[2 * rows :, 128:] = result[4 * rows :, 128:]


def fresh(gain, w_key, w_value, pools0, pools1, rows):
    sources = [*pools0, *pools1[2:]]
    width = gain.shape[1]
    return pl.pallas_call(
        fresh_body,
        out_shape=(jax.ShapeDtypeStruct((4 * rows, 256), BF16),) * 2,
        in_specs=vmem(9),
        out_specs=tuple(vmem(2)),
        scratch_shapes=[pltpu.VMEM((6 * rows, width), BF16)],
        compiler_params=pltpu.CompilerParams(vmem_limit_bytes=FRE * MIB),
        cost_estimate=pl.CostEstimate(flops=10**9, bytes_accessed=2 * MIB, transcendentals=0),
        name="fresh",
    )(gain, w_key, w_value, *sources)


def attend_body(slots, *refs):
    ids, queries = refs[:2]
    pool = refs[2:10]
    k_new, v_new, out = refs[10:]
    rows = queries.shape[0]
    fresh_rows = k_new.shape[0]
    each = fresh_rows // 4
    scale = 0.125 * math.log2(math.e)
    me = ids[0]
    chip = lax.rem(lax.div(me, 2), 4)
    beyond = lax.rem(chip + 2 * lax.rem(chip, 2) + 3, 4)
    partners = (jnp.bitwise_xor(me, 2), me + 2 * (beyond - chip))
    key_lane = lane_iota((rows, fresh_rows))
    row = lax.broadcasted_iota(jnp.int32, (rows, fresh_rows), 0)
    row_pos = each * (4 * (row // each) + lax.rem(me, 4)) + row % each
    lane = lane_iota((rows, 128))
    stats = jnp.zeros((rows, 128), F32)
    for head in range(2):
        partner = partners[head]
        slot = key_lane // each
        owner = jnp.bitwise_xor(jnp.where(slot < 2, me, partner), slot % 2)
        allowed = each * owner + key_lane % each <= row_pos
        cols = slice(head * 128, (head + 1) * 128)
        q = queries[:, cols].astype(F32)
        places = range(4 * head, 4 * head + 4)
        for which in range(2):
            combo = 2 * head + which
            kept = (lane < 64) if which == 0 else (lane >= 64)
            masked = jnp.where(kept, q, 0.0).astype(BF16)
            scores = [nt_dot(masked, pool[i][0, :slots]) for i in places]
            last = jnp.where(allowed, nt_dot(masked, k_new[:, cols]), NEG)
            row_max = jnp.max(last, axis=-1, keepdims=True)
            for s in scores:
                row_max = jnp.maximum(row_max, jnp.max(s, axis=-1, keepdims=True))
            weights = jnp.exp2((last - row_max) * scale)
            total = jnp.sum(weights, axis=-1, keepdims=True)
            mixed = nn_dot(weights.astype(BF16), v_new[:, cols])
            for s, i in zip(scores, places):
                weights = jnp.exp2((s - row_max) * scale)
                total = total + jnp.sum(weights, axis=-1, keepdims=True)
                mixed = mixed + nn_dot(weights.astype(BF16), pool[i][1, :slots])
            mixed = mixed / total
            out[:, combo * 128 : (combo + 1) * 128] = mixed.astype(BF16)
            for base, stat in ((0, row_max), (4, total)):
                for part in range(3):
                    piece = stat.astype(BF16).astype(F32)
                    stats = jnp.where(lane == 8 * part + base + combo, piece, stats)
                    stat = stat - piece
    out[:, 512:640] = stats.astype(BF16)


def attend(ids, queries, pools0, pools1, slots, k_new, v_new):
    rows = queries.shape[0]
    keys = 4 * slots + k_new.shape[0]
    return pl.pallas_call(
        lambda *refs: attend_body(slots, *refs),
        out_shape=jax.ShapeDtypeStruct((rows, 640), BF16),
        in_specs=[pl.BlockSpec(memory_space=pltpu.SMEM)] + vmem(11),
        out_specs=vmem(1)[0],
        compiler_params=pltpu.CompilerParams(vmem_limit_bytes=ATT * MIB),
        cost_estimate=pl.CostEstimate(
            flops=4 * rows * keys * 512, bytes_accessed=2 * MIB, transcendentals=4 * rows * keys
        ),
        name="attend",
    )(ids, queries, *pools0, *pools1, k_new, v_new)


def combine_body(parts, dec_out, lambdas, head_gain, out):
    scale = 0.125 * math.log2(math.e)
    members = parts.shape[0]
    rows = parts.shape[1]

    def whole(member):
        pieces = parts[member, :, 512:640].astype(F32)
        return pieces + pltpu.roll(pieces, 120, 1) + pltpu.roll(pieces, 112, 1)

    stats = [whole(member) for member in range(members)]
    top = stats[0]
    for s in stats[1:]:
        top = jnp.maximum(top, s)
    shares = [jnp.exp2((s - top) * scale) * pltpu.roll(s, 124, 1) for s in stats]
    total = shares[0]
    for s in shares[1:]:
        total = total + s
    sums = []
    for combo in range(4):
        acc = jnp.zeros((rows, 128), F32)
        for member in range(members):
            acc = acc + shares[member][:, combo : combo + 1] * parts[
                member, :, combo * 128 : (combo + 1) * 128
            ].astype(F32)
        sums.append(acc / total[:, combo : combo + 1])
    heads = []
    for head in range(2):
        attended = sums[2 * head] - lambdas[head] * sums[2 * head + 1]
        heads.append(rms(attended, head_gain[...]).astype(BF16))
    for copy in range(out.shape[0]):
        for head in range(2):
            out[copy, :rows, head * 128 : (head + 1) * 128] = heads[head]
        out[copy, rows:, :] = jnp.broadcast_to(dec_out[...], (out.shape[1] - rows, 256))


def combine(parts, dec_out, lambdas, head_gain, copies):
    return pl.pallas_call(
        combine_body,
        out_shape=jax.ShapeDtypeStruct((copies, parts.shape[1] + 8, 256), BF16),
        in_specs=vmem(2) + [pl.BlockSpec(memory_space=pltpu.SMEM)] + vmem(1),
        out_specs=vmem(1)[0],
        compiler_params=pltpu.CompilerParams(vmem_limit_bytes=16 * MIB),
        cost_estimate=pl.CostEstimate(flops=10**8, bytes_accessed=MIB, transcendentals=0),
        name="combine",
    )(parts, dec_out, lambdas, head_gain)


def out_body(heads, w, piece, dec):
    rows = piece.shape[0]
    acc = nn_dot(heads[0], w[:256])
    for copy in range(1, heads.shape[0]):
        acc = acc + nn_dot(heads[copy], w[copy * 256 : (copy + 1) * 256])
    piece[...] = acc[:rows].astype(BF16)
    dec[...] = acc[rows : rows + 1].astype(BF16)


def out_rows(heads, w, rows):
    return pl.pallas_call(
        out_body,
        out_shape=(
            jax.ShapeDtypeStruct((rows, w.shape[1]), BF16),
            jax.ShapeDtypeStruct((1, w.shape[1]), BF16),
        ),
        in_specs=vmem(2),
        out_specs=tuple(vmem(2)),
        compiler_params=pltpu.CompilerParams(vmem_limit_bytes=8 * MIB),
        cost_estimate=pl.CostEstimate(flops=10**8, bytes_accessed=MIB, transcendentals=0),
        name="out_rows",
    )(heads, w)


def layer(
    x_piece,
    x_decode,
    norm_gain,
    w_query,
    w_key,
    w_value,
    w_out,
    head_gain,
    lambdas,
    piece_keys,
    piece_values,
    cache_keys,
    cache_values,
    cache_lengths,
):
    kv_count = lax.axis_size("kv")
    tp_count = lax.axis_size("tp")
    members = kv_count // SHARE
    rows = x_piece.shape[0]
    groups = [[SHARE * m + e for m in range(members)] for e in range(SHARE)]
    gain = norm_gain.reshape(1, -1)
    head_gain = head_gain.reshape(1, -1)
    me = lax.axis_index("kv")

    def across(i):
        chip = i // 2 % 4
        return i + 2 * ((chip + 2 * (chip % 2) + 3) % 4 - chip)

    ids = me.reshape(1)

    def move(array, target):
        return lax.ppermute(array, "kv", [(i, target(i)) for i in range(kv_count)])

    pool0, pool1, sent, q_dec = opening(
        piece_keys.reshape(-1, 128),
        piece_values.reshape(-1, 128),
        x_piece,
        x_decode,
        gain,
        w_query,
        members,
    )
    far0 = move(pool0, lambda i: i ^ 2)
    far1 = move(pool1, across)
    pools0 = [pool0, move(pool0, lambda i: i ^ 1), far0]
    pools1 = [pool1, move(pool1, lambda i: i ^ 1), far1]
    pools0.append(move(far0, lambda i: i ^ 1))
    pools1.append(move(far1, lambda i: i ^ 1))
    got = lax.all_to_all(sent, "kv", 0, 0, tiled=True, axis_index_groups=groups)
    dec_out = decode(
        x_decode,
        gain,
        w_key,
        w_value,
        q_dec,
        cache_keys.reshape(-1, 128),
        cache_values.reshape(-1, 128),
        cache_lengths,
        lambdas,
        head_gain,
    )
    k_new, v_new = fresh(gain, w_key, w_value, pools0, pools1, rows)
    slots = piece_keys.shape[0]
    parts = attend(
        ids, got.reshape(members * rows, 256), pools0, pools1, slots, k_new, v_new
    )
    parts = lax.all_to_all(
        parts.reshape(members, rows, 640), "kv", 0, 0, tiled=True, axis_index_groups=groups
    )
    heads = combine(parts, dec_out, lambdas, head_gain, tp_count)
    heads = lax.all_to_all(heads, "tp", 0, 0, tiled=True)
    return out_rows(heads, w_out, rows)


def solution(mesh):
    placed = (
        P("kv", None),
        P("kv", None),
        P(),
        P(None, "tp"),
        P(None, "tp"),
        P(None, "tp"),
        P(None, "tp"),
        P(),
        P("tp"),
        P("kv", "tp", None),
        P("kv", "tp", None),
        P("kv", None, "tp", None),
        P("kv", None, "tp", None),
        P("kv"),
    )
    return jax.shard_map(
        layer,
        mesh=mesh,
        in_specs=placed,
        out_specs=(P("kv", "tp"), P("kv", "tp")),
        check_vma=False,
    )
```

```python
import math

import jax
import jax.numpy as jnp
from jax import lax
from jax.experimental import pallas as pl
from jax.experimental.pallas import tpu as pltpu
from jax.sharding import PartitionSpec as P

EPS = 1e-06
SHARE = 4
NEG = -jnp.inf
F32 = jnp.float32
BF16 = jnp.bfloat16
MIB = 1024 * 1024
ATT, FRE, DEC, OPN = 20, 8, 16, 60


def nt_dot(a, b):
    return lax.dot_general(a, b, (((1,), (1,)), ((), ())), preferred_element_type=F32)


def nn_dot(a, b):
    return lax.dot_general(a, b, (((1,), (0,)), ((), ())), preferred_element_type=F32)


def lane_iota(shape):
    return lax.broadcasted_iota(jnp.int32, shape, len(shape) - 1)


def rms(rows, gain):
    return rows * lax.rsqrt(jnp.mean(rows * rows, axis=-1, keepdims=True) + EPS) * gain


def vmem(count):
    return [pl.BlockSpec(memory_space=pltpu.VMEM)] * count


HBM = pl.BlockSpec(memory_space=pltpu.HBM)


def fetch(pairs, sems):
    copies = [pltpu.make_async_copy(a, b, sems.at[i]) for i, (a, b) in enumerate(pairs)]
    for copy in copies:
        copy.start()
    return copies


def opening_body(
    keys, values, x, x_dec, gain, w, pool0, pool1, out, out_dec, kv, xs, xd, g, wq, wide, normed, sems
):
    pools = (pool0, pool1)
    copies = fetch(
        (
            (x, xs),
            (x_dec, xd),
            (gain, g),
            (keys, kv.at[0]),
            (values, kv.at[1]),
            (w, wq),
        ),
        sems,
    )
    slots = keys.shape[0] // 2
    rows = x.shape[0]
    for copy in copies[:3]:
        copy.wait()
    normed[:rows] = rms(xs[...].astype(F32), g[...]).astype(BF16)
    normed[rows:] = jnp.broadcast_to(
        rms(xd[...].astype(F32), g[...]).astype(BF16), (16, x.shape[1])
    )
    for tile in range(x.shape[1] // 128):
        at = slots + rows * (tile // 2)
        for pool in pools:
            pool[tile % 2, at : at + rows, :] = xs[:, tile * 128 : (tile + 1) * 128]
    for index in range(2):
        copies[3 + index].wait()
        wide[index] = kv[index].astype(F32)
        for head in range(2):
            pools[head][index, :slots] = wide[index, pl.ds(head, slots, stride=2), :].astype(BF16)
    copies[5].wait()
    result = nn_dot(normed[...], wq[...]).astype(BF16)
    for member in range(out.shape[0]):
        out[member] = result[:rows]
    out_dec[...] = result[rows : rows + 1]


def opening(keys, values, x, x_dec, gain, w, members):
    rows, width = x.shape
    slots = keys.shape[0] // 2
    return pl.pallas_call(
        opening_body,
        out_shape=(
            pltpu.VMEM((2, slots + rows * width // 256, 128), BF16),
            pltpu.VMEM((2, slots + rows * width // 256, 128), BF16),
            pltpu.VMEM((members, rows, w.shape[1]), BF16),
            jax.ShapeDtypeStruct((1, w.shape[1]), BF16),
        ),
        in_specs=[HBM] * 6,
        out_specs=tuple(vmem(4)),
        scratch_shapes=[
            pltpu.VMEM((2, 2 * slots, 128), BF16),
            pltpu.VMEM((rows, width), BF16),
            pltpu.VMEM((1, width), BF16),
            pltpu.VMEM((1, width), F32),
            pltpu.VMEM(w.shape, BF16),
            pltpu.VMEM((2, 2 * slots, 128), F32),
            pltpu.VMEM((rows + 16, width), BF16),
            pltpu.SemaphoreType.DMA((6,)),
        ],
        compiler_params=pltpu.CompilerParams(vmem_limit_bytes=OPN * MIB),
        cost_estimate=pl.CostEstimate(flops=10**9, bytes_accessed=2 * MIB, transcendentals=0),
        name="opening",
    )(keys, values, x, x_dec, gain, w)


def decode_body(
    x_dec, gain, w_key, w_value, q_dec, keys, values, length, lambdas, head_gain, head_out,
    xd, g, wk, wv, kc, vc, sems
):
    copies = fetch(
        ((x_dec, xd), (gain, g), (w_key, wk), (keys, kc), (w_value, wv), (values, vc)), sems
    )
    for copy in copies[:2]:
        copy.wait()
    normed = jnp.broadcast_to(rms(xd[...].astype(F32), g[...]).astype(BF16), (16, xd.shape[1]))
    copies[2].wait()
    new_keys = nn_dot(normed, wk[...]).astype(BF16)[:1]

    row = lax.broadcasted_iota(jnp.int32, (8, 128), 0)
    lane = lane_iota((8, 128))
    second = (row // 2) % 2 == 1

    def per_head(line):
        line = line.astype(F32)
        return jnp.where(
            second,
            jnp.broadcast_to(line[:, 128:], (8, 128)),
            jnp.broadcast_to(line[:, :128], (8, 128)),
        )

    half = lane // 64 == row % 2
    queries = jnp.where(half, per_head(q_dec[...]), 0.0)
    own_keys = per_head(new_keys)
    scale = 0.125 * math.log2(math.e)
    copies[3].wait()
    scores = nt_dot(queries.astype(BF16), kc[...])
    width = keys.shape[0]
    column = lane_iota((8, width))
    wide_row = lax.broadcasted_iota(jnp.int32, (8, width), 0)
    allowed = (column % 2 == (wide_row // 2) % 2) & (column // 2 < length[0])
    scores = jnp.where(allowed, scores, NEG)
    own_score = jnp.sum(queries * own_keys, axis=-1, keepdims=True)
    row_max = jnp.maximum(jnp.max(scores, axis=-1, keepdims=True), own_score)
    weights = jnp.exp2((scores - row_max) * scale)
    own_weight = jnp.exp2((own_score - row_max) * scale)
    totals = jnp.sum(weights, axis=-1, keepdims=True) + own_weight
    copies[4].wait()
    own_values = per_head(nn_dot(normed, wv[...]).astype(BF16)[:1])
    copies[5].wait()
    mixed = nn_dot(weights.astype(BF16), vc[...])
    mixed = (mixed + own_weight.astype(BF16).astype(F32) * own_values) / totals
    for head in range(2):
        attended = mixed[2 * head : 2 * head + 1] - lambdas[head] * mixed[2 * head + 1 : 2 * head + 2]
        head_out[:, head * 128 : (head + 1) * 128] = rms(attended, head_gain[...]).astype(BF16)


def decode(x_dec, gain, w_key, w_value, q_dec, keys, values, length, lambdas, head_gain):
    smem = pl.BlockSpec(memory_space=pltpu.SMEM)
    return pl.pallas_call(
        decode_body,
        out_shape=jax.ShapeDtypeStruct((1, 256), BF16),
        in_specs=[HBM] * 4 + vmem(1) + [HBM] * 2 + [smem, smem] + vmem(1),
        out_specs=vmem(1)[0],
        scratch_shapes=[
            pltpu.VMEM(x_dec.shape, BF16),
            pltpu.VMEM(gain.shape, F32),
            pltpu.VMEM(w_key.shape, BF16),
            pltpu.VMEM(w_value.shape, BF16),
            pltpu.VMEM(keys.shape, BF16),
            pltpu.VMEM(values.shape, BF16),
            pltpu.SemaphoreType.DMA((6,)),
        ],
        compiler_params=pltpu.CompilerParams(vmem_limit_bytes=DEC * MIB),
        cost_estimate=pl.CostEstimate(flops=2 * 10**9, bytes_accessed=4 * MIB, transcendentals=0),
        name="decode",
    )(x_dec, gain, w_key, w_value, q_dec, keys, values, length, lambdas, head_gain)


def fresh_body(*refs):
    gain, w_key, w_value = refs[:3]
    sources = refs[3:9]
    k_out, v_out, normed = refs[9:]
    rows = k_out.shape[0] // 4
    tiles = gain.shape[1] // 128
    slots = sources[0].shape[1] - rows * tiles // 2
    for index, source in enumerate(sources):
        parts = [
            source[tile % 2, slots + rows * (tile // 2) : slots + rows * (tile // 2 + 1), :]
            for tile in range(tiles)
        ]
        x = jnp.concatenate(parts, axis=1).astype(F32)
        normed[index * rows : (index + 1) * rows] = rms(x, gain[...]).astype(BF16)
    for w, out in ((w_key, k_out), (w_value, v_out)):
        result = nn_dot(normed[...], w[...]).astype(BF16)
        out[:, :128] = result[: 4 * rows, :128]
        out[: 2 * rows, 128:] = result[: 2 * rows, 128:]
        out[2 * rows :, 128:] = result[4 * rows :, 128:]


def fresh(gain, w_key, w_value, pools0, pools1, rows):
    sources = [*pools0, *pools1[2:]]
    width = gain.shape[1]
    return pl.pallas_call(
        fresh_body,
        out_shape=(jax.ShapeDtypeStruct((4 * rows, 256), BF16),) * 2,
        in_specs=vmem(9),
        out_specs=tuple(vmem(2)),
        scratch_shapes=[pltpu.VMEM((6 * rows, width), BF16)],
        compiler_params=pltpu.CompilerParams(vmem_limit_bytes=FRE * MIB),
        cost_estimate=pl.CostEstimate(flops=10**9, bytes_accessed=2 * MIB, transcendentals=0),
        name="fresh",
    )(gain, w_key, w_value, *sources)


def attend_body(slots, *refs):
    ids, queries = refs[:2]
    pool = refs[2:10]
    k_new, v_new, out = refs[10:]
    rows = queries.shape[0]
    fresh_rows = k_new.shape[0]
    each = fresh_rows // 4
    scale = 0.125 * math.log2(math.e)
    me = ids[0]
    chip = lax.rem(lax.div(me, 2), 4)
    beyond = lax.rem(chip + 2 * lax.rem(chip, 2) + 3, 4)
    partners = (jnp.bitwise_xor(me, 2), me + 2 * (beyond - chip))
    key_lane = lane_iota((rows, fresh_rows))
    row = lax.broadcasted_iota(jnp.int32, (rows, fresh_rows), 0)
    row_pos = each * (4 * (row // each) + lax.rem(me, 4)) + row % each
    lane = lane_iota((rows, 128))
    stats = jnp.zeros((rows, 128), F32)
    for head in range(2):
        partner = partners[head]
        slot = key_lane // each
        owner = jnp.bitwise_xor(jnp.where(slot < 2, me, partner), slot % 2)
        allowed = each * owner + key_lane % each <= row_pos
        cols = slice(head * 128, (head + 1) * 128)
        q = queries[:, cols].astype(F32)
        places = range(4 * head, 4 * head + 4)
        for which in range(2):
            combo = 2 * head + which
            kept = (lane < 64) if which == 0 else (lane >= 64)
            masked = jnp.where(kept, q, 0.0).astype(BF16)
            scores = [nt_dot(masked, pool[i][0, :slots]) for i in places]
            last = jnp.where(allowed, nt_dot(masked, k_new[:, cols]), NEG)
            row_max = jnp.max(last, axis=-1, keepdims=True)
            for s in scores:
                row_max = jnp.maximum(row_max, jnp.max(s, axis=-1, keepdims=True))
            weights = jnp.exp2((last - row_max) * scale)
            total = jnp.sum(weights, axis=-1, keepdims=True)
            mixed = nn_dot(weights.astype(BF16), v_new[:, cols])
            for s, i in zip(scores, places):
                weights = jnp.exp2((s - row_max) * scale)
                total = total + jnp.sum(weights, axis=-1, keepdims=True)
                mixed = mixed + nn_dot(weights.astype(BF16), pool[i][1, :slots])
            mixed = mixed / total
            out[:, combo * each : (combo + 1) * each, :] = mixed.astype(BF16).reshape(
                rows // each, each, 128
            )
            for base, stat in ((0, row_max), (4, total)):
                for part in range(3):
                    piece = stat.astype(BF16).astype(F32)
                    stats = jnp.where(lane % 64 == 8 * part + base + combo, piece, stats)
                    stat = stat - piece
    stats = stats.reshape(rows // each, 2, each // 2, 128)
    low = lane_iota((rows // each, each // 2, 128)) < 64
    out[:, 4 * each :, :] = jnp.where(low, stats[:, 0], stats[:, 1]).astype(BF16)


def attend(ids, queries, pools0, pools1, slots, k_new, v_new):
    rows = queries.shape[0]
    keys = 4 * slots + k_new.shape[0]
    each = k_new.shape[0] // 4
    return pl.pallas_call(
        lambda *refs: attend_body(slots, *refs),
        out_shape=pltpu.HBM((rows // each, 4 * each + each // 2, 128), BF16),
        in_specs=[pl.BlockSpec(memory_space=pltpu.SMEM)] + vmem(11),
        out_specs=vmem(1)[0],
        compiler_params=pltpu.CompilerParams(vmem_limit_bytes=ATT * MIB),
        cost_estimate=pl.CostEstimate(
            flops=4 * rows * keys * 512, bytes_accessed=2 * MIB, transcendentals=4 * rows * keys
        ),
        name="attend",
    )(ids, queries, *pools0, *pools1, k_new, v_new)


def combine_body(parts, dec_out, lambdas, head_gain, out):
    scale = 0.125 * math.log2(math.e)
    members = parts.shape[0]
    rows = parts.shape[1] * 2 // 9

    def whole(member):
        pieces = parts[member, 4 * rows :, :].astype(F32)
        pieces = jnp.concatenate([pieces, pltpu.roll(pieces, 64, 1)], axis=0)
        return pieces + pltpu.roll(pieces, 120, 1) + pltpu.roll(pieces, 112, 1)

    stats = [whole(member) for member in range(members)]
    top = stats[0]
    for s in stats[1:]:
        top = jnp.maximum(top, s)
    shares = [jnp.exp2((s - top) * scale) * pltpu.roll(s, 124, 1) for s in stats]
    total = shares[0]
    for s in shares[1:]:
        total = total + s
    sums = []
    for combo in range(4):
        acc = jnp.zeros((rows, 128), F32)
        for member in range(members):
            acc = acc + shares[member][:, combo : combo + 1] * parts[
                member, combo * rows : (combo + 1) * rows, :
            ].astype(F32)
        sums.append(acc / total[:, combo : combo + 1])
    heads = []
    for head in range(2):
        attended = sums[2 * head] - lambdas[head] * sums[2 * head + 1]
        heads.append(rms(attended, head_gain[...]).astype(BF16))
    for copy in range(out.shape[0]):
        for head in range(2):
            out[copy, :rows, head * 128 : (head + 1) * 128] = heads[head]
        out[copy, rows:, :] = jnp.broadcast_to(dec_out[...], (out.shape[1] - rows, 256))


def combine(parts, dec_out, lambdas, head_gain, copies):
    rows = parts.shape[1] * 2 // 9
    return pl.pallas_call(
        combine_body,
        out_shape=jax.ShapeDtypeStruct((copies, rows + 8, 256), BF16),
        in_specs=vmem(2) + [pl.BlockSpec(memory_space=pltpu.SMEM)] + vmem(1),
        out_specs=vmem(1)[0],
        compiler_params=pltpu.CompilerParams(vmem_limit_bytes=16 * MIB),
        cost_estimate=pl.CostEstimate(flops=10**8, bytes_accessed=MIB, transcendentals=0),
        name="combine",
    )(parts, dec_out, lambdas, head_gain)


def own_body(place, heads, w, out):
    start = pl.multiple_of(place[0] * 256, 256)
    out[...] = nn_dot(heads[0], w[pl.ds(start, 256), :])


def own_rows(place, heads, w):
    return pl.pallas_call(
        own_body,
        out_shape=jax.ShapeDtypeStruct((heads.shape[1], w.shape[1]), F32),
        in_specs=[pl.BlockSpec(memory_space=pltpu.SMEM)] + vmem(2),
        out_specs=vmem(1)[0],
        compiler_params=pltpu.CompilerParams(vmem_limit_bytes=8 * MIB),
        cost_estimate=pl.CostEstimate(flops=10**9, bytes_accessed=MIB, transcendentals=0),
        name="own_rows",
    )(place, heads, w)


def out_body(place, own, heads, w, piece, dec):
    rows = piece.shape[0]
    count = heads.shape[0]
    acc = own[...]
    for step in range(1, count):
        other = lax.rem(place[0] + step, count)
        start = pl.multiple_of(other * 256, 256)
        acc = acc + nn_dot(heads[other], w[pl.ds(start, 256), :])
    piece[...] = acc[:rows].astype(BF16)
    dec[...] = acc[rows : rows + 1].astype(BF16)


def out_rows(place, own, heads, w, rows):
    return pl.pallas_call(
        out_body,
        out_shape=(
            jax.ShapeDtypeStruct((rows, w.shape[1]), BF16),
            jax.ShapeDtypeStruct((1, w.shape[1]), BF16),
        ),
        in_specs=[pl.BlockSpec(memory_space=pltpu.SMEM)] + vmem(3),
        out_specs=tuple(vmem(2)),
        compiler_params=pltpu.CompilerParams(vmem_limit_bytes=8 * MIB),
        cost_estimate=pl.CostEstimate(flops=10**8, bytes_accessed=MIB, transcendentals=0),
        name="out_rows",
    )(place, own, heads, w)


def layer(
    x_piece,
    x_decode,
    norm_gain,
    w_query,
    w_key,
    w_value,
    w_out,
    head_gain,
    lambdas,
    piece_keys,
    piece_values,
    cache_keys,
    cache_values,
    cache_lengths,
):
    kv_count = lax.axis_size("kv")
    tp_count = lax.axis_size("tp")
    members = kv_count // SHARE
    rows = x_piece.shape[0]
    groups = [[SHARE * m + e for m in range(members)] for e in range(SHARE)]
    gain = norm_gain.reshape(1, -1)
    head_gain = head_gain.reshape(1, -1)
    me = lax.axis_index("kv")

    def across(i):
        chip = i // 2 % 4
        return i + 2 * ((chip + 2 * (chip % 2) + 3) % 4 - chip)

    ids = me.reshape(1)

    def move(array, target):
        return lax.ppermute(array, "kv", [(i, target(i)) for i in range(kv_count)])

    pool0, pool1, sent, q_dec = opening(
        piece_keys.reshape(-1, 128),
        piece_values.reshape(-1, 128),
        x_piece,
        x_decode,
        gain,
        w_query,
        members,
    )
    far0 = move(pool0, lambda i: i ^ 2)
    far1 = move(pool1, across)
    pools0 = [pool0, move(pool0, lambda i: i ^ 1), far0]
    pools1 = [pool1, move(pool1, lambda i: i ^ 1), far1]
    pools0.append(move(far0, lambda i: i ^ 1))
    pools1.append(move(far1, lambda i: i ^ 1))
    got = lax.all_to_all(sent, "kv", 0, 0, tiled=True, axis_index_groups=groups)
    dec_out = decode(
        x_decode,
        gain,
        w_key,
        w_value,
        q_dec,
        cache_keys.reshape(-1, 128),
        cache_values.reshape(-1, 128),
        cache_lengths,
        lambdas,
        head_gain,
    )
    k_new, v_new = fresh(gain, w_key, w_value, pools0, pools1, rows)
    slots = piece_keys.shape[0]
    parts = attend(
        ids, got.reshape(members * rows, 256), pools0, pools1, slots, k_new, v_new
    )
    parts = lax.all_to_all(
        parts, "kv", 0, 0, tiled=True, axis_index_groups=groups
    )
    heads = combine(parts, dec_out, lambdas, head_gain, tp_count)
    place = lax.axis_index("tp").reshape(1)
    own = own_rows(place, heads, w_out)
    heads = lax.all_to_all(heads, "tp", 0, 0, tiled=True)
    return out_rows(place, own, heads, w_out, rows)


def solution(mesh):
    placed = (
        P("kv", None),
        P("kv", None),
        P(),
        P(None, "tp"),
        P(None, "tp"),
        P(None, "tp"),
        P(None, "tp"),
        P(),
        P("tp"),
        P("kv", "tp", None),
        P("kv", "tp", None),
        P("kv", None, "tp", None),
        P("kv", None, "tp", None),
        P("kv"),
    )
    return jax.shard_map(
        layer,
        mesh=mesh,
        in_specs=placed,
        out_specs=(P("kv", "tp"), P("kv", "tp")),
        check_vma=False,
    )
```

```python
import math

import jax
import jax.numpy as jnp
from jax import lax
from jax.experimental import pallas as pl
from jax.experimental.pallas import tpu as pltpu
from jax.sharding import PartitionSpec as P

EPS = 1e-06
SHARE = 4
NEG = -jnp.inf
F32 = jnp.float32
BF16 = jnp.bfloat16
MIB = 1024 * 1024
ATT, FRE, DEC, OPN = 20, 8, 60, 60


def nt_dot(a, b):
    return lax.dot_general(a, b, (((1,), (1,)), ((), ())), preferred_element_type=F32)


def nn_dot(a, b):
    return lax.dot_general(a, b, (((1,), (0,)), ((), ())), preferred_element_type=F32)


def lane_iota(shape):
    return lax.broadcasted_iota(jnp.int32, shape, len(shape) - 1)


def rms(rows, gain):
    return rows * lax.rsqrt(jnp.mean(rows * rows, axis=-1, keepdims=True) + EPS) * gain


def vmem(count):
    return [pl.BlockSpec(memory_space=pltpu.VMEM)] * count


HBM = pl.BlockSpec(memory_space=pltpu.HBM)


def fetch(pairs, sems):
    copies = [pltpu.make_async_copy(a, b, sems.at[i]) for i, (a, b) in enumerate(pairs)]
    for copy in copies:
        copy.start()
    return copies


def opening_body(
    keys, values, x, x_dec, gain, w, pool0, pool1, out, out_dec, row_dec, kv, xs, xd, g, wq, wide, normed,
    sems
):
    pools = (pool0, pool1)
    copies = fetch(
        (
            (x, xs),
            (x_dec, xd),
            (gain, g),
            (keys, kv.at[0]),
            (values, kv.at[1]),
            (w, wq),
        ),
        sems,
    )
    slots = keys.shape[0] // 2
    rows = x.shape[0]
    for copy in copies[:3]:
        copy.wait()
    normed[:rows] = rms(xs[...].astype(F32), g[...]).astype(BF16)
    normed[rows:] = jnp.broadcast_to(
        rms(xd[...].astype(F32), g[...]).astype(BF16), (16, x.shape[1])
    )
    row_dec[...] = normed[rows : rows + 1]
    for tile in range(x.shape[1] // 128):
        at = slots + rows * (tile // 2)
        for pool in pools:
            pool[tile % 2, at : at + rows, :] = normed[:rows, tile * 128 : (tile + 1) * 128]
    for index in range(2):
        copies[3 + index].wait()
        wide[index] = kv[index].astype(F32)
        for head in range(2):
            pools[head][index, :slots] = wide[index, pl.ds(head, slots, stride=2), :].astype(BF16)
    copies[5].wait()
    result = nn_dot(normed[...], wq[...]).astype(BF16)
    for member in range(out.shape[0]):
        out[member] = result[:rows]
    out_dec[...] = result[rows : rows + 1]


def opening(keys, values, x, x_dec, gain, w, members):
    rows, width = x.shape
    slots = keys.shape[0] // 2
    return pl.pallas_call(
        opening_body,
        out_shape=(
            pltpu.VMEM((2, slots + rows * width // 256, 128), BF16),
            pltpu.VMEM((2, slots + rows * width // 256, 128), BF16),
            pltpu.VMEM((members, rows, w.shape[1]), BF16),
            jax.ShapeDtypeStruct((1, w.shape[1]), BF16),
            jax.ShapeDtypeStruct((1, width), BF16),
        ),
        in_specs=[HBM] * 6,
        out_specs=tuple(vmem(5)),
        scratch_shapes=[
            pltpu.VMEM((2, 2 * slots, 128), BF16),
            pltpu.VMEM((rows, width), BF16),
            pltpu.VMEM((1, width), BF16),
            pltpu.VMEM((1, width), F32),
            pltpu.VMEM(w.shape, BF16),
            pltpu.VMEM((2, 2 * slots, 128), F32),
            pltpu.VMEM((rows + 16, width), BF16),
            pltpu.SemaphoreType.DMA((6,)),
        ],
        compiler_params=pltpu.CompilerParams(vmem_limit_bytes=OPN * MIB),
        cost_estimate=pl.CostEstimate(flops=10**9, bytes_accessed=2 * MIB, transcendentals=0),
        name="opening",
    )(keys, values, x, x_dec, gain, w)


def decode_body(
    q_dec, k_dec, v_dec, keys, values, length, lambdas, head_gain, head_out, kc, vc, sems
):
    copies = fetch(((keys, kc), (values, vc)), sems)

    row = lax.broadcasted_iota(jnp.int32, (8, 128), 0)
    lane = lane_iota((8, 128))
    second = (row // 2) % 2 == 1

    def per_head(line):
        line = line.astype(F32)
        return jnp.where(
            second,
            jnp.broadcast_to(line[:, 128:], (8, 128)),
            jnp.broadcast_to(line[:, :128], (8, 128)),
        )

    half = lane // 64 == row % 2
    queries = jnp.where(half, per_head(q_dec[...]), 0.0)
    own_keys = per_head(k_dec[...])
    own_values = per_head(v_dec[...])
    scale = 0.125 * math.log2(math.e)
    copies[0].wait()
    scores = nt_dot(queries.astype(BF16), kc[...])
    width = keys.shape[0]
    column = lane_iota((8, width))
    wide_row = lax.broadcasted_iota(jnp.int32, (8, width), 0)
    allowed = (column % 2 == (wide_row // 2) % 2) & (column // 2 < length[0])
    scores = jnp.where(allowed, scores, NEG)
    own_score = jnp.sum(queries * own_keys, axis=-1, keepdims=True)
    row_max = jnp.maximum(jnp.max(scores, axis=-1, keepdims=True), own_score)
    weights = jnp.exp2((scores - row_max) * scale)
    own_weight = jnp.exp2((own_score - row_max) * scale)
    totals = jnp.sum(weights, axis=-1, keepdims=True) + own_weight
    copies[1].wait()
    mixed = nn_dot(weights.astype(BF16), vc[...])
    mixed = (mixed + own_weight.astype(BF16).astype(F32) * own_values) / totals
    for head in range(2):
        attended = mixed[2 * head : 2 * head + 1] - lambdas[head] * mixed[2 * head + 1 : 2 * head + 2]
        head_out[:, head * 128 : (head + 1) * 128] = rms(attended, head_gain[...]).astype(BF16)


def decode(q_dec, k_dec, v_dec, keys, values, length, lambdas, head_gain):
    smem = pl.BlockSpec(memory_space=pltpu.SMEM)
    return pl.pallas_call(
        decode_body,
        out_shape=pltpu.VMEM((1, 256), BF16),
        in_specs=vmem(3) + [HBM] * 2 + [smem, smem] + vmem(1),
        out_specs=vmem(1)[0],
        scratch_shapes=[
            pltpu.VMEM(keys.shape, BF16),
            pltpu.VMEM(values.shape, BF16),
            pltpu.SemaphoreType.DMA((2,)),
        ],
        compiler_params=pltpu.CompilerParams(vmem_limit_bytes=DEC * MIB),
        cost_estimate=pl.CostEstimate(flops=2 * 10**9, bytes_accessed=2 * MIB, transcendentals=0),
        name="decode",
    )(q_dec, k_dec, v_dec, keys, values, length, lambdas, head_gain)


def fresh_body(*refs):
    row_dec, w_key, w_value = refs[:3]
    sources = refs[3:9]
    k_out, v_out, k_dec, v_dec, xs, normed, sems = refs[9:]
    rows = k_out.shape[0] // 4
    tiles = row_dec.shape[1] // 128
    slots = sources[0].shape[1] - rows * tiles // 2
    copies = fetch([(s.at[:, slots:], xs.at[i]) for i, s in enumerate(sources)], sems)
    normed[6 * rows :] = jnp.broadcast_to(row_dec[...], (16, row_dec.shape[1]))
    for index in range(6):
        copies[index].wait()
        for tile in range(tiles):
            normed[index * rows : (index + 1) * rows, tile * 128 : (tile + 1) * 128] = xs[
                index, tile % 2, rows * (tile // 2) : rows * (tile // 2 + 1), :
            ]
    for w, out, out_dec in ((w_key, k_out, k_dec), (w_value, v_out, v_dec)):
        result = nn_dot(normed[...], w[...]).astype(BF16)
        out[:, :128] = result[: 4 * rows, :128]
        out[: 2 * rows, 128:] = result[: 2 * rows, 128:]
        out[2 * rows :, 128:] = result[4 * rows : 6 * rows, 128:]
        out_dec[...] = result[6 * rows : 6 * rows + 1]


def fresh(row_dec, w_key, w_value, pools0, pools1, rows):
    sources = [*pools0, *pools1[2:]]
    width = row_dec.shape[1]
    return pl.pallas_call(
        fresh_body,
        out_shape=(
            jax.ShapeDtypeStruct((4 * rows, 256), BF16),
            jax.ShapeDtypeStruct((4 * rows, 256), BF16),
            jax.ShapeDtypeStruct((1, 256), BF16),
            jax.ShapeDtypeStruct((1, 256), BF16),
        ),
        in_specs=vmem(3) + [HBM] * 6,
        out_specs=tuple(vmem(4)),
        scratch_shapes=[
            pltpu.VMEM((6, 2, rows * width // 256, 128), BF16),
            pltpu.VMEM((6 * rows + 16, width), BF16),
            pltpu.SemaphoreType.DMA((6,)),
        ],
        compiler_params=pltpu.CompilerParams(vmem_limit_bytes=FRE * MIB),
        cost_estimate=pl.CostEstimate(flops=10**9, bytes_accessed=2 * MIB, transcendentals=0),
        name="fresh",
    )(row_dec, w_key, w_value, *sources)


def attend_body(slots, *refs):
    ids, queries = refs[:2]
    sources = refs[2:10]
    k_new, v_new, out, pool, sems = refs[10:]
    copies = fetch([(s.at[:, :slots], pool.at[i]) for i, s in enumerate(sources)], sems)
    rows = queries.shape[0]
    fresh_rows = k_new.shape[0]
    each = fresh_rows // 4
    scale = 0.125 * math.log2(math.e)
    me = ids[0]
    chip = lax.rem(lax.div(me, 2), 4)
    beyond = lax.rem(chip + 2 * lax.rem(chip, 2) + 3, 4)
    partners = (jnp.bitwise_xor(me, 2), me + 2 * (beyond - chip))
    key_lane = lane_iota((rows, fresh_rows))
    row = lax.broadcasted_iota(jnp.int32, (rows, fresh_rows), 0)
    row_pos = each * (4 * (row // each) + lax.rem(me, 4)) + row % each
    lane = lane_iota((rows, 128))
    stats = jnp.zeros((rows, 128), F32)
    for head in range(2):
        partner = partners[head]
        slot = key_lane // each
        owner = jnp.bitwise_xor(jnp.where(slot < 2, me, partner), slot % 2)
        allowed = each * owner + key_lane % each <= row_pos
        cols = slice(head * 128, (head + 1) * 128)
        q = queries[:, cols].astype(F32)
        places = range(4 * head, 4 * head + 4)
        for i in places:
            copies[i].wait()
        for which in range(2):
            combo = 2 * head + which
            kept = (lane < 64) if which == 0 else (lane >= 64)
            masked = jnp.where(kept, q, 0.0).astype(BF16)
            scores = [nt_dot(masked, pool[i, 0]) for i in places]
            last = jnp.where(allowed, nt_dot(masked, k_new[:, cols]), NEG)
            row_max = jnp.max(last, axis=-1, keepdims=True)
            for s in scores:
                row_max = jnp.maximum(row_max, jnp.max(s, axis=-1, keepdims=True))
            weights = jnp.exp2((last - row_max) * scale)
            total = jnp.sum(weights, axis=-1, keepdims=True)
            mixed = nn_dot(weights.astype(BF16), v_new[:, cols])
            for s, i in zip(scores, places):
                weights = jnp.exp2((s - row_max) * scale)
                total = total + jnp.sum(weights, axis=-1, keepdims=True)
                mixed = mixed + nn_dot(weights.astype(BF16), pool[i, 1])
            mixed = mixed / total
            out[:, combo * each : (combo + 1) * each, :] = mixed.astype(BF16).reshape(
                rows // each, each, 128
            )
            for base, stat in ((0, row_max), (4, total)):
                for part in range(3):
                    piece = stat.astype(BF16).astype(F32)
                    stats = jnp.where(lane % 64 == 8 * part + base + combo, piece, stats)
                    stat = stat - piece
    stats = stats.reshape(rows // each, 2, each // 2, 128)
    low = lane_iota((rows // each, each // 2, 128)) < 64
    out[:, 4 * each :, :] = jnp.where(low, stats[:, 0], stats[:, 1]).astype(BF16)


def attend(ids, queries, pools0, pools1, slots, k_new, v_new):
    rows = queries.shape[0]
    keys = 4 * slots + k_new.shape[0]
    each = k_new.shape[0] // 4
    return pl.pallas_call(
        lambda *refs: attend_body(slots, *refs),
        out_shape=pltpu.HBM((rows // each, 4 * each + each // 2, 128), BF16),
        in_specs=[pl.BlockSpec(memory_space=pltpu.SMEM)] + vmem(1) + [HBM] * 8 + vmem(2),
        out_specs=vmem(1)[0],
        scratch_shapes=[
            pltpu.VMEM((8, 2, slots, 128), BF16),
            pltpu.SemaphoreType.DMA((8,)),
        ],
        compiler_params=pltpu.CompilerParams(vmem_limit_bytes=ATT * MIB),
        cost_estimate=pl.CostEstimate(
            flops=4 * rows * keys * 512, bytes_accessed=2 * MIB, transcendentals=4 * rows * keys
        ),
        name="attend",
    )(ids, queries, *pools0, *pools1, k_new, v_new)


def combine_body(parts, dec_out, lambdas, head_gain, out):
    scale = 0.125 * math.log2(math.e)
    members = parts.shape[0]
    rows = parts.shape[1] * 2 // 9

    def whole(member):
        pieces = parts[member, 4 * rows :, :].astype(F32)
        pieces = jnp.concatenate([pieces, pltpu.roll(pieces, 64, 1)], axis=0)
        return pieces + pltpu.roll(pieces, 120, 1) + pltpu.roll(pieces, 112, 1)

    stats = [whole(member) for member in range(members)]
    top = stats[0]
    for s in stats[1:]:
        top = jnp.maximum(top, s)
    shares = [jnp.exp2((s - top) * scale) * pltpu.roll(s, 124, 1) for s in stats]
    total = shares[0]
    for s in shares[1:]:
        total = total + s
    sums = []
    for combo in range(4):
        acc = jnp.zeros((rows, 128), F32)
        for member in range(members):
            acc = acc + shares[member][:, combo : combo + 1] * parts[
                member, combo * rows : (combo + 1) * rows, :
            ].astype(F32)
        sums.append(acc / total[:, combo : combo + 1])
    heads = []
    for head in range(2):
        attended = sums[2 * head] - lambdas[head] * sums[2 * head + 1]
        heads.append(rms(attended, head_gain[...]).astype(BF16))
    for copy in range(out.shape[0]):
        for head in range(2):
            out[copy, :rows, head * 128 : (head + 1) * 128] = heads[head]
        out[copy, rows:, :] = jnp.broadcast_to(dec_out[...], (out.shape[1] - rows, 256))


def combine(parts, dec_out, lambdas, head_gain, copies):
    rows = parts.shape[1] * 2 // 9
    return pl.pallas_call(
        combine_body,
        out_shape=jax.ShapeDtypeStruct((copies, rows + 8, 256), BF16),
        in_specs=vmem(2) + [pl.BlockSpec(memory_space=pltpu.SMEM)] + vmem(1),
        out_specs=vmem(1)[0],
        compiler_params=pltpu.CompilerParams(vmem_limit_bytes=16 * MIB),
        cost_estimate=pl.CostEstimate(flops=10**8, bytes_accessed=MIB, transcendentals=0),
        name="combine",
    )(parts, dec_out, lambdas, head_gain)


def out_body(heads, w, piece, dec):
    rows = piece.shape[0]
    acc = nn_dot(heads[0], w[:256])
    for copy in range(1, heads.shape[0]):
        acc = acc + nn_dot(heads[copy], w[copy * 256 : (copy + 1) * 256])
    piece[...] = acc[:rows].astype(BF16)
    dec[...] = acc[rows : rows + 1].astype(BF16)


def out_rows(heads, w, rows):
    return pl.pallas_call(
        out_body,
        out_shape=(
            jax.ShapeDtypeStruct((rows, w.shape[1]), BF16),
            jax.ShapeDtypeStruct((1, w.shape[1]), BF16),
        ),
        in_specs=vmem(2),
        out_specs=tuple(vmem(2)),
        compiler_params=pltpu.CompilerParams(vmem_limit_bytes=8 * MIB),
        cost_estimate=pl.CostEstimate(flops=10**8, bytes_accessed=MIB, transcendentals=0),
        name="out_rows",
    )(heads, w)


def layer(
    x_piece,
    x_decode,
    norm_gain,
    w_query,
    w_key,
    w_value,
    w_out,
    head_gain,
    lambdas,
    piece_keys,
    piece_values,
    cache_keys,
    cache_values,
    cache_lengths,
):
    kv_count = lax.axis_size("kv")
    tp_count = lax.axis_size("tp")
    members = kv_count // SHARE
    rows = x_piece.shape[0]
    groups = [[SHARE * m + e for m in range(members)] for e in range(SHARE)]
    gain = norm_gain.reshape(1, -1)
    head_gain = head_gain.reshape(1, -1)
    me = lax.axis_index("kv")

    def across(i):
        chip = i // 2 % 4
        return i + 2 * ((chip + 2 * (chip % 2) + 3) % 4 - chip)

    ids = me.reshape(1)

    def move(array, target):
        return lax.ppermute(array, "kv", [(i, target(i)) for i in range(kv_count)])

    pool0, pool1, sent, q_dec, row_dec = opening(
        piece_keys.reshape(-1, 128),
        piece_values.reshape(-1, 128),
        x_piece,
        x_decode,
        gain,
        w_query,
        members,
    )
    far0 = move(pool0, lambda i: i ^ 2)
    far1 = move(pool1, across)
    pools0 = [pool0, move(pool0, lambda i: i ^ 1), far0]
    pools1 = [pool1, move(pool1, lambda i: i ^ 1), far1]
    pools0.append(move(far0, lambda i: i ^ 1))
    pools1.append(move(far1, lambda i: i ^ 1))
    got = lax.all_to_all(sent, "kv", 0, 0, tiled=True, axis_index_groups=groups)
    k_new, v_new, k_dec, v_dec = fresh(row_dec, w_key, w_value, pools0, pools1, rows)
    dec_out = decode(
        q_dec,
        k_dec,
        v_dec,
        cache_keys.reshape(-1, 128),
        cache_values.reshape(-1, 128),
        cache_lengths,
        lambdas,
        head_gain,
    )
    slots = piece_keys.shape[0]
    parts = attend(
        ids, got.reshape(members * rows, 256), pools0, pools1, slots, k_new, v_new
    )
    parts = lax.all_to_all(
        parts, "kv", 0, 0, tiled=True, axis_index_groups=groups
    )
    heads = combine(parts, dec_out, lambdas, head_gain, tp_count)
    heads = lax.all_to_all(heads, "tp", 0, 0, tiled=True)
    return out_rows(heads, w_out, rows)


def solution(mesh):
    placed = (
        P("kv", None),
        P("kv", None),
        P(),
        P(None, "tp"),
        P(None, "tp"),
        P(None, "tp"),
        P(None, "tp"),
        P(),
        P("tp"),
        P("kv", "tp", None),
        P("kv", "tp", None),
        P("kv", None, "tp", None),
        P("kv", None, "tp", None),
        P("kv"),
    )
    return jax.shard_map(
        layer,
        mesh=mesh,
        in_specs=placed,
        out_specs=(P("kv", "tp"), P("kv", "tp")),
        check_vma=False,
    )
```

```python
import math

import jax
import jax.numpy as jnp
from jax import lax
from jax.experimental import pallas as pl
from jax.experimental.pallas import tpu as pltpu
from jax.sharding import PartitionSpec as P

EPS = 1e-06
SHARE = 4
NEG = -jnp.inf
F32 = jnp.float32
BF16 = jnp.bfloat16
MIB = 1024 * 1024
ATT, FRE, DEC, OPN = 20, 8, 60, 60


def nt_dot(a, b):
    return lax.dot_general(a, b, (((1,), (1,)), ((), ())), preferred_element_type=F32)


def nn_dot(a, b):
    return lax.dot_general(a, b, (((1,), (0,)), ((), ())), preferred_element_type=F32)


def lane_iota(shape):
    return lax.broadcasted_iota(jnp.int32, shape, len(shape) - 1)


def rms(rows, gain):
    return rows * lax.rsqrt(jnp.mean(rows * rows, axis=-1, keepdims=True) + EPS) * gain


def vmem(count):
    return [pl.BlockSpec(memory_space=pltpu.VMEM)] * count


HBM = pl.BlockSpec(memory_space=pltpu.HBM)


def fetch(pairs, sems):
    copies = [pltpu.make_async_copy(a, b, sems.at[i]) for i, (a, b) in enumerate(pairs)]
    for copy in copies:
        copy.start()
    return copies


def opening_body(
    keys, values, x, x_dec, gain, w, pool, out, out_dec, row_dec, kv, xs, xd, g, wq, wide, normed,
    sems
):

    copies = fetch(
        (
            (x, xs),
            (x_dec, xd),
            (gain, g),
            (keys, kv.at[0]),
            (values, kv.at[1]),
            (w, wq),
        ),
        sems,
    )
    slots = keys.shape[0] // 2
    rows = x.shape[0]
    for copy in copies[:3]:
        copy.wait()
    normed[:rows] = rms(xs[...].astype(F32), g[...]).astype(BF16)
    normed[rows:] = jnp.broadcast_to(
        rms(xd[...].astype(F32), g[...]).astype(BF16), (16, x.shape[1])
    )
    row_dec[...] = normed[rows : rows + 1]
    for tile in range(x.shape[1] // 128):
        at = slots + rows * (tile // 4)
        pool[tile % 4, at : at + rows, :] = normed[:rows, tile * 128 : (tile + 1) * 128]
    for index in range(2):
        copies[3 + index].wait()
        wide[index] = kv[index].astype(F32)
        for head in range(2):
            pool[2 * head + index, :slots] = wide[index, pl.ds(head, slots, stride=2), :].astype(
                BF16
            )
    copies[5].wait()
    result = nn_dot(normed[...], wq[...]).astype(BF16)
    for member in range(out.shape[0]):
        out[member] = result[:rows]
    out_dec[...] = result[rows : rows + 1]


def opening(keys, values, x, x_dec, gain, w, members):
    rows, width = x.shape
    slots = keys.shape[0] // 2
    return pl.pallas_call(
        opening_body,
        out_shape=(
            pltpu.VMEM((4, slots + rows * width // 512, 128), BF16),
            pltpu.VMEM((members, rows, w.shape[1]), BF16),
            jax.ShapeDtypeStruct((1, w.shape[1]), BF16),
            jax.ShapeDtypeStruct((1, width), BF16),
        ),
        in_specs=[HBM] * 6,
        out_specs=tuple(vmem(4)),
        scratch_shapes=[
            pltpu.VMEM((2, 2 * slots, 128), BF16),
            pltpu.VMEM((rows, width), BF16),
            pltpu.VMEM((1, width), BF16),
            pltpu.VMEM((1, width), F32),
            pltpu.VMEM(w.shape, BF16),
            pltpu.VMEM((2, 2 * slots, 128), F32),
            pltpu.VMEM((rows + 16, width), BF16),
            pltpu.SemaphoreType.DMA((6,)),
        ],
        compiler_params=pltpu.CompilerParams(vmem_limit_bytes=OPN * MIB),
        cost_estimate=pl.CostEstimate(flops=10**9, bytes_accessed=2 * MIB, transcendentals=0),
        name="opening",
    )(keys, values, x, x_dec, gain, w)


def decode_body(
    q_dec, k_dec, v_dec, keys, values, length, lambdas, head_gain, head_out, kc, vc, sems
):
    copies = fetch(((keys, kc), (values, vc)), sems)

    row = lax.broadcasted_iota(jnp.int32, (8, 128), 0)
    lane = lane_iota((8, 128))
    second = (row // 2) % 2 == 1

    def per_head(line):
        line = line.astype(F32)
        return jnp.where(
            second,
            jnp.broadcast_to(line[:, 128:], (8, 128)),
            jnp.broadcast_to(line[:, :128], (8, 128)),
        )

    half = lane // 64 == row % 2
    queries = jnp.where(half, per_head(q_dec[...]), 0.0)
    own_keys = per_head(k_dec[...])
    own_values = per_head(v_dec[...])
    scale = 0.125 * math.log2(math.e)
    copies[0].wait()
    scores = nt_dot(queries.astype(BF16), kc[...])
    width = keys.shape[0]
    column = lane_iota((8, width))
    wide_row = lax.broadcasted_iota(jnp.int32, (8, width), 0)
    allowed = (column % 2 == (wide_row // 2) % 2) & (column // 2 < length[0])
    scores = jnp.where(allowed, scores, NEG)
    own_score = jnp.sum(queries * own_keys, axis=-1, keepdims=True)
    row_max = jnp.maximum(jnp.max(scores, axis=-1, keepdims=True), own_score)
    weights = jnp.exp2((scores - row_max) * scale)
    own_weight = jnp.exp2((own_score - row_max) * scale)
    totals = jnp.sum(weights, axis=-1, keepdims=True) + own_weight
    copies[1].wait()
    mixed = nn_dot(weights.astype(BF16), vc[...])
    mixed = (mixed + own_weight.astype(BF16).astype(F32) * own_values) / totals
    for head in range(2):
        attended = mixed[2 * head : 2 * head + 1] - lambdas[head] * mixed[2 * head + 1 : 2 * head + 2]
        head_out[:, head * 128 : (head + 1) * 128] = rms(attended, head_gain[...]).astype(BF16)


def decode(q_dec, k_dec, v_dec, keys, values, length, lambdas, head_gain):
    smem = pl.BlockSpec(memory_space=pltpu.SMEM)
    return pl.pallas_call(
        decode_body,
        out_shape=pltpu.VMEM((1, 256), BF16),
        in_specs=vmem(3) + [HBM] * 2 + [smem, smem] + vmem(1),
        out_specs=vmem(1)[0],
        scratch_shapes=[
            pltpu.VMEM(keys.shape, BF16),
            pltpu.VMEM(values.shape, BF16),
            pltpu.SemaphoreType.DMA((2,)),
        ],
        compiler_params=pltpu.CompilerParams(vmem_limit_bytes=DEC * MIB),
        cost_estimate=pl.CostEstimate(flops=2 * 10**9, bytes_accessed=2 * MIB, transcendentals=0),
        name="decode",
    )(q_dec, k_dec, v_dec, keys, values, length, lambdas, head_gain)


def fresh_body(*refs):
    row_dec, w_key, w_value = refs[:3]
    pools = refs[3:7]
    k_out, v_out, k_dec, v_dec, xs, normed, sems = refs[7:]
    total = k_out.shape[0]
    rows = total // 4
    tiles = row_dec.shape[1] // 128
    slots = pools[0].shape[1] - rows * tiles // 4
    copies = fetch([(s.at[:, slots:], xs.at[i]) for i, s in enumerate(pools)], sems)
    normed[total:] = jnp.broadcast_to(row_dec[...], (16, row_dec.shape[1]))
    for index in range(4):
        copies[index].wait()
        for tile in range(tiles):
            normed[index * rows : (index + 1) * rows, tile * 128 : (tile + 1) * 128] = xs[
                index, tile % 4, rows * (tile // 4) : rows * (tile // 4 + 1), :
            ]
    for w, out, out_dec in ((w_key, k_out, k_dec), (w_value, v_out, v_dec)):
        result = nn_dot(normed[...], w[...]).astype(BF16)
        out[...] = result[:total]
        out_dec[...] = result[total : total + 1]


def fresh(row_dec, w_key, w_value, pools, rows):
    width = row_dec.shape[1]
    return pl.pallas_call(
        fresh_body,
        out_shape=(
            jax.ShapeDtypeStruct((4 * rows, 256), BF16),
            jax.ShapeDtypeStruct((4 * rows, 256), BF16),
            jax.ShapeDtypeStruct((1, 256), BF16),
            jax.ShapeDtypeStruct((1, 256), BF16),
        ),
        in_specs=vmem(3) + [HBM] * 4,
        out_specs=tuple(vmem(4)),
        scratch_shapes=[
            pltpu.VMEM((4, 4, rows * width // 512, 128), BF16),
            pltpu.VMEM((4 * rows + 16, width), BF16),
            pltpu.SemaphoreType.DMA((4,)),
        ],
        compiler_params=pltpu.CompilerParams(vmem_limit_bytes=FRE * MIB),
        cost_estimate=pl.CostEstimate(flops=10**9, bytes_accessed=2 * MIB, transcendentals=0),
        name="fresh",
    )(row_dec, w_key, w_value, *pools)


def attend_body(slots, *refs):
    ids, queries = refs[:2]
    sources = refs[2:6]
    k_new, v_new, out, pool, sems = refs[6:]
    copies = fetch(
        [
            (source.at[2 * head : 2 * head + 2, :slots], pool.at[i, 2 * head : 2 * head + 2])
            for head in range(2)
            for i, source in enumerate(sources)
        ],
        sems,
    )
    rows = queries.shape[0]
    fresh_rows = k_new.shape[0]
    each = fresh_rows // 4
    scale = 0.125 * math.log2(math.e)
    block = min(128, rows)
    me = ids[0]
    core = lax.rem(me, 2)
    chip = lax.rem(lax.div(me, 2), 4)
    beyond = lax.rem(chip + 2 * lax.rem(chip, 2) + 3, 4)
    first = jnp.bitwise_xor(me - core, 2)
    second = me - core + 1 + 2 * (beyond - chip)
    key_lane = lane_iota((block, fresh_rows))
    slot = key_lane // each
    owner = jnp.where(
        slot < 2,
        jnp.bitwise_xor(me, slot % 2),
        jnp.where(jnp.bitwise_xor(core, slot % 2) == 0, first, second),
    )
    key_pos = each * owner + key_lane % each
    row = lax.broadcasted_iota(jnp.int32, (block, fresh_rows), 0)
    lane = lane_iota((block, 128))

    def score(task):
        head, which, start = task
        if which == 0 and start == 0:
            for copy in copies[4 * head : 4 * head + 4]:
                copy.wait()
        cols = slice(head * 128, (head + 1) * 128)
        q = queries[start : start + block, cols].astype(F32)
        kept = (lane < 64) if which == 0 else (lane >= 64)
        masked = jnp.where(kept, q, 0.0).astype(BF16)
        at = row + start
        row_pos = each * (4 * (at // each) + lax.rem(me, 4)) + at % each
        last = jnp.where(key_pos <= row_pos, nt_dot(masked, k_new[:, cols]), NEG)
        return [nt_dot(masked, pool[i, 2 * head]) for i in range(4)], last

    stats = {start: jnp.zeros((block, 128), F32) for start in range(0, rows, block)}

    def finish(task, scores, last):
        head, which, start = task
        combo = 2 * head + which
        row_max = jnp.max(last, axis=-1, keepdims=True)
        for s in scores:
            row_max = jnp.maximum(row_max, jnp.max(s, axis=-1, keepdims=True))
        weights = jnp.exp2((last - row_max) * scale)
        total = jnp.sum(weights, axis=-1, keepdims=True)
        mixed = nn_dot(weights.astype(BF16), v_new[:, head * 128 : (head + 1) * 128])
        for i, s in enumerate(scores):
            weights = jnp.exp2((s - row_max) * scale)
            total = total + jnp.sum(weights, axis=-1, keepdims=True)
            mixed = mixed + nn_dot(weights.astype(BF16), pool[i, 2 * head + 1])
        mixed = mixed / total
        place = slice(start // each, (start + block) // each)
        out[place, combo * each : (combo + 1) * each, :] = mixed.astype(BF16).reshape(
            block // each, each, 128
        )
        for base, stat in ((0, row_max), (4, total)):
            for part in range(3):
                piece = stat.astype(BF16).astype(F32)
                at = lane % 64 == 8 * part + base + combo
                stats[start] = jnp.where(at, piece, stats[start])
                stat = stat - piece

    tasks = [(h, w, start) for h in range(2) for w in range(2) for start in range(0, rows, block)]
    ahead = score(tasks[0])
    for index, task in enumerate(tasks):
        ready = ahead
        if index + 1 < len(tasks):
            ahead = score(tasks[index + 1])
        finish(task, *ready)
    low = lane_iota((block // each, each // 2, 128)) < 64
    for start in range(0, rows, block):
        pair = stats[start].reshape(block // each, 2, each // 2, 128)
        place = slice(start // each, (start + block) // each)
        out[place, 4 * each :, :] = jnp.where(low, pair[:, 0], pair[:, 1]).astype(BF16)


def attend(ids, queries, pools, slots, k_new, v_new):
    rows = queries.shape[0]
    keys = 4 * slots + k_new.shape[0]
    each = k_new.shape[0] // 4
    return pl.pallas_call(
        lambda *refs: attend_body(slots, *refs),
        out_shape=pltpu.HBM((rows // each, 4 * each + each // 2, 128), BF16),
        in_specs=[pl.BlockSpec(memory_space=pltpu.SMEM)] + vmem(1) + [HBM] * 4 + vmem(2),
        out_specs=vmem(1)[0],
        scratch_shapes=[
            pltpu.VMEM((4, 4, slots, 128), BF16),
            pltpu.SemaphoreType.DMA((8,)),
        ],
        compiler_params=pltpu.CompilerParams(vmem_limit_bytes=ATT * MIB),
        cost_estimate=pl.CostEstimate(
            flops=4 * rows * keys * 512, bytes_accessed=2 * MIB, transcendentals=4 * rows * keys
        ),
        name="attend",
    )(ids, queries, *pools, k_new, v_new)


def combine_body(parts, dec_out, lambdas, head_gain, out):
    scale = 0.125 * math.log2(math.e)
    members = parts.shape[0]
    rows = parts.shape[1] * 2 // 9

    def whole(member):
        pieces = parts[member, 4 * rows :, :].astype(F32)
        pieces = jnp.concatenate([pieces, pltpu.roll(pieces, 64, 1)], axis=0)
        return pieces + pltpu.roll(pieces, 120, 1) + pltpu.roll(pieces, 112, 1)

    stats = [whole(member) for member in range(members)]
    top = stats[0]
    for s in stats[1:]:
        top = jnp.maximum(top, s)
    shares = [jnp.exp2((s - top) * scale) * pltpu.roll(s, 124, 1) for s in stats]
    total = shares[0]
    for s in shares[1:]:
        total = total + s
    sums = []
    for combo in range(4):
        acc = jnp.zeros((rows, 128), F32)
        for member in range(members):
            acc = acc + shares[member][:, combo : combo + 1] * parts[
                member, combo * rows : (combo + 1) * rows, :
            ].astype(F32)
        sums.append(acc / total[:, combo : combo + 1])
    heads = []
    for head in range(2):
        attended = sums[2 * head] - lambdas[head] * sums[2 * head + 1]
        heads.append(rms(attended, head_gain[...]).astype(BF16))
    for copy in range(out.shape[0]):
        for head in range(2):
            out[copy, :rows, head * 128 : (head + 1) * 128] = heads[head]
        out[copy, rows:, :] = jnp.broadcast_to(dec_out[...], (out.shape[1] - rows, 256))


def combine(parts, dec_out, lambdas, head_gain, copies):
    rows = parts.shape[1] * 2 // 9
    return pl.pallas_call(
        combine_body,
        out_shape=jax.ShapeDtypeStruct((copies, rows + 8, 256), BF16),
        in_specs=vmem(2) + [pl.BlockSpec(memory_space=pltpu.SMEM)] + vmem(1),
        out_specs=vmem(1)[0],
        compiler_params=pltpu.CompilerParams(vmem_limit_bytes=16 * MIB),
        cost_estimate=pl.CostEstimate(flops=10**8, bytes_accessed=MIB, transcendentals=0),
        name="combine",
    )(parts, dec_out, lambdas, head_gain)


def out_body(heads, w, piece, dec):
    rows = piece.shape[0]
    acc = nn_dot(heads[0], w[:256])
    for copy in range(1, heads.shape[0]):
        acc = acc + nn_dot(heads[copy], w[copy * 256 : (copy + 1) * 256])
    piece[...] = acc[:rows].astype(BF16)
    dec[...] = acc[rows : rows + 1].astype(BF16)


def out_rows(heads, w, rows):
    return pl.pallas_call(
        out_body,
        out_shape=(
            jax.ShapeDtypeStruct((rows, w.shape[1]), BF16),
            jax.ShapeDtypeStruct((1, w.shape[1]), BF16),
        ),
        in_specs=vmem(2),
        out_specs=tuple(vmem(2)),
        compiler_params=pltpu.CompilerParams(vmem_limit_bytes=8 * MIB),
        cost_estimate=pl.CostEstimate(flops=10**8, bytes_accessed=MIB, transcendentals=0),
        name="out_rows",
    )(heads, w)


def layer(
    x_piece,
    x_decode,
    norm_gain,
    w_query,
    w_key,
    w_value,
    w_out,
    head_gain,
    lambdas,
    piece_keys,
    piece_values,
    cache_keys,
    cache_values,
    cache_lengths,
):
    kv_count = lax.axis_size("kv")
    tp_count = lax.axis_size("tp")
    members = kv_count // SHARE
    rows = x_piece.shape[0]
    groups = [[SHARE * m + e for m in range(members)] for e in range(SHARE)]
    gain = norm_gain.reshape(1, -1)
    head_gain = head_gain.reshape(1, -1)
    me = lax.axis_index("kv")

    def across(i):
        chip = i // 2 % 4
        if i % 2 == 0:
            return i ^ 2
        return i + 2 * ((chip + 2 * (chip % 2) + 3) % 4 - chip)

    ids = me.reshape(1)

    def move(array, target):
        return lax.ppermute(array, "kv", [(i, target(i)) for i in range(kv_count)])

    pool, sent, q_dec, row_dec = opening(
        piece_keys.reshape(-1, 128),
        piece_values.reshape(-1, 128),
        x_piece,
        x_decode,
        gain,
        w_query,
        members,
    )
    far = move(pool, across)
    pools = [pool, move(pool, lambda i: i ^ 1), far, move(far, lambda i: i ^ 1)]
    got = lax.all_to_all(sent, "kv", 0, 0, tiled=True, axis_index_groups=groups)
    k_new, v_new, k_dec, v_dec = fresh(row_dec, w_key, w_value, pools, rows)
    dec_out = decode(
        q_dec,
        k_dec,
        v_dec,
        cache_keys.reshape(-1, 128),
        cache_values.reshape(-1, 128),
        cache_lengths,
        lambdas,
        head_gain,
    )
    slots = piece_keys.shape[0]
    parts = attend(ids, got.reshape(members * rows, 256), pools, slots, k_new, v_new)
    parts = lax.all_to_all(
        parts, "kv", 0, 0, tiled=True, axis_index_groups=groups
    )
    heads = combine(parts, dec_out, lambdas, head_gain, tp_count)
    heads = lax.all_to_all(heads, "tp", 0, 0, tiled=True)
    return out_rows(heads, w_out, rows)


def solution(mesh):
    placed = (
        P("kv", None),
        P("kv", None),
        P(),
        P(None, "tp"),
        P(None, "tp"),
        P(None, "tp"),
        P(None, "tp"),
        P(),
        P("tp"),
        P("kv", "tp", None),
        P("kv", "tp", None),
        P("kv", None, "tp", None),
        P("kv", None, "tp", None),
        P("kv"),
    )
    return jax.shard_map(
        layer,
        mesh=mesh,
        in_specs=placed,
        out_specs=(P("kv", "tp"), P("kv", "tp")),
        check_vma=False,
    )
```

```python
import math

import jax
import jax.numpy as jnp
from jax import lax
from jax.experimental import pallas as pl
from jax.experimental.pallas import tpu as pltpu
from jax.sharding import PartitionSpec as P

EPS = 1e-06
SHARE = 4
NEG = -jnp.inf
F32 = jnp.float32
BF16 = jnp.bfloat16
MIB = 1024 * 1024
ATT, FRE, DEC, OPN = 20, 8, 60, 60


def nt_dot(a, b):
    return lax.dot_general(a, b, (((1,), (1,)), ((), ())), preferred_element_type=F32)


def nn_dot(a, b):
    return lax.dot_general(a, b, (((1,), (0,)), ((), ())), preferred_element_type=F32)


def lane_iota(shape):
    return lax.broadcasted_iota(jnp.int32, shape, len(shape) - 1)


def rms(rows, gain):
    return rows * lax.rsqrt(jnp.mean(rows * rows, axis=-1, keepdims=True) + EPS) * gain


def vmem(count):
    return [pl.BlockSpec(memory_space=pltpu.VMEM)] * count


HBM = pl.BlockSpec(memory_space=pltpu.HBM)


def fetch(pairs, sems):
    copies = [pltpu.make_async_copy(a, b, sems.at[i]) for i, (a, b) in enumerate(pairs)]
    for copy in copies:
        copy.start()
    return copies


def opening_body(
    keys, values, x, x_dec, gain, w, pool, out, out_dec, row_dec, kv, xs, xd, g, wq, wide, normed,
    sems
):

    copies = fetch(
        (
            (x, xs),
            (x_dec, xd),
            (gain, g),
            (keys, kv.at[0]),
            (values, kv.at[1]),
            (w, wq),
        ),
        sems,
    )
    slots = keys.shape[0] // 2
    rows = x.shape[0]
    for copy in copies[:3]:
        copy.wait()
    normed[:rows] = rms(xs[...].astype(F32), g[...]).astype(BF16)
    normed[rows:] = jnp.broadcast_to(
        rms(xd[...].astype(F32), g[...]).astype(BF16), (16, x.shape[1])
    )
    row_dec[...] = normed[rows : rows + 1]
    for tile in range(x.shape[1] // 128):
        at = slots + rows * (tile // 4)
        pool[tile % 4, at : at + rows, :] = normed[:rows, tile * 128 : (tile + 1) * 128]
    for index in range(2):
        copies[3 + index].wait()
        wide[index] = kv[index].astype(F32)
        for head in range(2):
            pool[2 * head + index, :slots] = wide[index, pl.ds(head, slots, stride=2), :].astype(
                BF16
            )
    copies[5].wait()
    result = nn_dot(normed[...], wq[...]).astype(BF16)
    for member in range(out.shape[0]):
        out[member] = result[:rows]
    out_dec[...] = result[rows : rows + 1]


def opening(keys, values, x, x_dec, gain, w, members):
    rows, width = x.shape
    slots = keys.shape[0] // 2
    return pl.pallas_call(
        opening_body,
        out_shape=(
            pltpu.VMEM((4, slots + rows * width // 512, 128), BF16),
            pltpu.VMEM((members, rows, w.shape[1]), BF16),
            jax.ShapeDtypeStruct((1, w.shape[1]), BF16),
            jax.ShapeDtypeStruct((1, width), BF16),
        ),
        in_specs=[HBM] * 6,
        out_specs=tuple(vmem(4)),
        scratch_shapes=[
            pltpu.VMEM((2, 2 * slots, 128), BF16),
            pltpu.VMEM((rows, width), BF16),
            pltpu.VMEM((1, width), BF16),
            pltpu.VMEM((1, width), F32),
            pltpu.VMEM(w.shape, BF16),
            pltpu.VMEM((2, 2 * slots, 128), F32),
            pltpu.VMEM((rows + 16, width), BF16),
            pltpu.SemaphoreType.DMA((6,)),
        ],
        compiler_params=pltpu.CompilerParams(vmem_limit_bytes=OPN * MIB),
        cost_estimate=pl.CostEstimate(flops=10**9, bytes_accessed=2 * MIB, transcendentals=0),
        name="opening",
    )(keys, values, x, x_dec, gain, w)


def decode_body(
    q_dec, k_dec, v_dec, keys, values, length, lambdas, head_gain, head_out, kc, vc, sems
):
    copies = fetch(((keys, kc), (values, vc)), sems)

    row = lax.broadcasted_iota(jnp.int32, (8, 128), 0)
    lane = lane_iota((8, 128))
    second = (row // 2) % 2 == 1

    def per_head(line):
        line = line.astype(F32)
        return jnp.where(
            second,
            jnp.broadcast_to(line[:, 128:], (8, 128)),
            jnp.broadcast_to(line[:, :128], (8, 128)),
        )

    half = lane // 64 == row % 2
    queries = jnp.where(half, per_head(q_dec[...]), 0.0)
    own_keys = per_head(k_dec[...])
    own_values = per_head(v_dec[...])
    scale = 0.125 * math.log2(math.e)
    copies[0].wait()
    scores = nt_dot(queries.astype(BF16), kc[...])
    width = keys.shape[0]
    column = lane_iota((8, width))
    wide_row = lax.broadcasted_iota(jnp.int32, (8, width), 0)
    allowed = (column % 2 == (wide_row // 2) % 2) & (column // 2 < length[0])
    scores = jnp.where(allowed, scores, NEG)
    own_score = jnp.sum(queries * own_keys, axis=-1, keepdims=True)
    row_max = jnp.maximum(jnp.max(scores, axis=-1, keepdims=True), own_score)
    weights = jnp.exp2((scores - row_max) * scale)
    own_weight = jnp.exp2((own_score - row_max) * scale)
    totals = jnp.sum(weights, axis=-1, keepdims=True) + own_weight
    copies[1].wait()
    mixed = nn_dot(weights.astype(BF16), vc[...])
    mixed = (mixed + own_weight.astype(BF16).astype(F32) * own_values) / totals
    for head in range(2):
        attended = mixed[2 * head : 2 * head + 1] - lambdas[head] * mixed[2 * head + 1 : 2 * head + 2]
        head_out[:, head * 128 : (head + 1) * 128] = rms(attended, head_gain[...]).astype(BF16)


def decode(q_dec, k_dec, v_dec, keys, values, length, lambdas, head_gain):
    smem = pl.BlockSpec(memory_space=pltpu.SMEM)
    return pl.pallas_call(
        decode_body,
        out_shape=pltpu.VMEM((1, 256), BF16),
        in_specs=vmem(3) + [HBM] * 2 + [smem, smem] + vmem(1),
        out_specs=vmem(1)[0],
        scratch_shapes=[
            pltpu.VMEM(keys.shape, BF16),
            pltpu.VMEM(values.shape, BF16),
            pltpu.SemaphoreType.DMA((2,)),
        ],
        compiler_params=pltpu.CompilerParams(vmem_limit_bytes=DEC * MIB),
        cost_estimate=pl.CostEstimate(flops=2 * 10**9, bytes_accessed=2 * MIB, transcendentals=0),
        name="decode",
    )(q_dec, k_dec, v_dec, keys, values, length, lambdas, head_gain)


def fresh_body(*refs):
    row_dec, w_key, w_value = refs[:3]
    pools = refs[3:7]
    k_out, v_out, k_dec, v_dec, xs, normed, sems = refs[7:]
    total = k_out.shape[0]
    rows = total // 4
    tiles = row_dec.shape[1] // 128
    slots = pools[0].shape[1] - rows * tiles // 4
    copies = fetch([(s.at[:, slots:], xs.at[i]) for i, s in enumerate(pools)], sems)
    normed[total:] = jnp.broadcast_to(row_dec[...], (16, row_dec.shape[1]))
    for index in range(4):
        copies[index].wait()
        for tile in range(tiles):
            normed[index * rows : (index + 1) * rows, tile * 128 : (tile + 1) * 128] = xs[
                index, tile % 4, rows * (tile // 4) : rows * (tile // 4 + 1), :
            ]
    for w, out, out_dec in ((w_key, k_out, k_dec), (w_value, v_out, v_dec)):
        result = nn_dot(normed[...], w[...]).astype(BF16)
        out[...] = result[:total]
        out_dec[...] = result[total : total + 1]


def fresh(row_dec, w_key, w_value, pools, rows):
    width = row_dec.shape[1]
    return pl.pallas_call(
        fresh_body,
        out_shape=(
            jax.ShapeDtypeStruct((4 * rows, 256), BF16),
            jax.ShapeDtypeStruct((4 * rows, 256), BF16),
            jax.ShapeDtypeStruct((1, 256), BF16),
            jax.ShapeDtypeStruct((1, 256), BF16),
        ),
        in_specs=vmem(3) + [HBM] * 4,
        out_specs=tuple(vmem(4)),
        scratch_shapes=[
            pltpu.VMEM((4, 4, rows * width // 512, 128), BF16),
            pltpu.VMEM((4 * rows + 16, width), BF16),
            pltpu.SemaphoreType.DMA((4,)),
        ],
        compiler_params=pltpu.CompilerParams(vmem_limit_bytes=FRE * MIB),
        cost_estimate=pl.CostEstimate(flops=10**9, bytes_accessed=2 * MIB, transcendentals=0),
        name="fresh",
    )(row_dec, w_key, w_value, *pools)


def attend_body(slots, *refs):
    ids, queries = refs[:2]
    sources = refs[2:6]
    k_new, v_new, out, pool, sems = refs[6:]
    copies = fetch(
        [
            (source.at[2 * head : 2 * head + 2, :slots], pool.at[i, 2 * head : 2 * head + 2])
            for head in range(2)
            for i, source in enumerate(sources)
        ],
        sems,
    )
    rows = queries.shape[0]
    fresh_rows = k_new.shape[0]
    each = fresh_rows // 4
    scale = 0.125 * math.log2(math.e)
    block = min(128, rows)
    me = ids[0]
    core = lax.rem(me, 2)
    y = lax.rem(lax.div(me, 2), 4)
    z = lax.div(me, 8)
    key_lane = lane_iota((block, fresh_rows))
    slot = key_lane // each
    of = jnp.bitwise_xor(core, slot % 2)
    z_of = jnp.where(of == 0, jnp.bitwise_xor(z, 1), lax.rem(z + 2 * lax.rem(z, 2) + 7, 8))
    owner = of + 2 * y + 8 * jnp.where(slot < 2, z, z_of)
    key_pos = each * owner + key_lane % each
    row = lax.broadcasted_iota(jnp.int32, (block, fresh_rows), 0)
    lane = lane_iota((block, 128))

    def score(task):
        head, which, start = task
        if which == 0 and start == 0:
            for copy in copies[4 * head : 4 * head + 4]:
                copy.wait()
        cols = slice(head * 128, (head + 1) * 128)
        q = queries[start : start + block, cols].astype(F32)
        kept = (lane < 64) if which == 0 else (lane >= 64)
        masked = jnp.where(kept, q, 0.0).astype(BF16)
        at = row + start
        member = at // each
        place = 8 * (2 * (member // 4) + lax.rem(z, 2)) + 2 * (member % 4) + core
        row_pos = each * place + at % each
        last = jnp.where(key_pos <= row_pos, nt_dot(masked, k_new[:, cols]), NEG)
        return [nt_dot(masked, pool[i, 2 * head]) for i in range(4)], last

    stats = {start: jnp.zeros((block, 128), F32) for start in range(0, rows, block)}

    def finish(task, scores, last):
        head, which, start = task
        combo = 2 * head + which
        row_max = jnp.max(last, axis=-1, keepdims=True)
        for s in scores:
            row_max = jnp.maximum(row_max, jnp.max(s, axis=-1, keepdims=True))
        weights = jnp.exp2((last - row_max) * scale)
        total = jnp.sum(weights, axis=-1, keepdims=True)
        mixed = nn_dot(weights.astype(BF16), v_new[:, head * 128 : (head + 1) * 128])
        for i, s in enumerate(scores):
            weights = jnp.exp2((s - row_max) * scale)
            total = total + jnp.sum(weights, axis=-1, keepdims=True)
            mixed = mixed + nn_dot(weights.astype(BF16), pool[i, 2 * head + 1])
        mixed = mixed / total
        place = slice(start // each, (start + block) // each)
        out[place, combo * each : (combo + 1) * each, :] = mixed.astype(BF16).reshape(
            block // each, each, 128
        )
        for base, stat in ((0, row_max), (4, total)):
            for part in range(3):
                piece = stat.astype(BF16).astype(F32)
                at = lane % 64 == 8 * part + base + combo
                stats[start] = jnp.where(at, piece, stats[start])
                stat = stat - piece

    tasks = [(h, w, start) for h in range(2) for w in range(2) for start in range(0, rows, block)]
    ahead = score(tasks[0])
    for index, task in enumerate(tasks):
        ready = ahead
        if index + 1 < len(tasks):
            ahead = score(tasks[index + 1])
        finish(task, *ready)
    low = lane_iota((block // each, each // 2, 128)) < 64
    for start in range(0, rows, block):
        pair = stats[start].reshape(block // each, 2, each // 2, 128)
        place = slice(start // each, (start + block) // each)
        out[place, 4 * each :, :] = jnp.where(low, pair[:, 0], pair[:, 1]).astype(BF16)


def attend(ids, queries, pools, slots, k_new, v_new):
    rows = queries.shape[0]
    keys = 4 * slots + k_new.shape[0]
    each = k_new.shape[0] // 4
    return pl.pallas_call(
        lambda *refs: attend_body(slots, *refs),
        out_shape=pltpu.HBM((rows // each, 4 * each + each // 2, 128), BF16),
        in_specs=[pl.BlockSpec(memory_space=pltpu.SMEM)] + vmem(1) + [HBM] * 4 + vmem(2),
        out_specs=vmem(1)[0],
        scratch_shapes=[
            pltpu.VMEM((4, 4, slots, 128), BF16),
            pltpu.SemaphoreType.DMA((8,)),
        ],
        compiler_params=pltpu.CompilerParams(vmem_limit_bytes=ATT * MIB),
        cost_estimate=pl.CostEstimate(
            flops=4 * rows * keys * 512, bytes_accessed=2 * MIB, transcendentals=4 * rows * keys
        ),
        name="attend",
    )(ids, queries, *pools, k_new, v_new)


def combine_body(parts, dec_out, lambdas, head_gain, out):
    scale = 0.125 * math.log2(math.e)
    members = parts.shape[0]
    rows = parts.shape[1] * 2 // 9

    def whole(member):
        pieces = parts[member, 4 * rows :, :].astype(F32)
        pieces = jnp.concatenate([pieces, pltpu.roll(pieces, 64, 1)], axis=0)
        return pieces + pltpu.roll(pieces, 120, 1) + pltpu.roll(pieces, 112, 1)

    stats = [whole(member) for member in range(members)]
    top = stats[0]
    for s in stats[1:]:
        top = jnp.maximum(top, s)
    shares = [jnp.exp2((s - top) * scale) * pltpu.roll(s, 124, 1) for s in stats]
    total = shares[0]
    for s in shares[1:]:
        total = total + s
    sums = []
    for combo in range(4):
        acc = jnp.zeros((rows, 128), F32)
        for member in range(members):
            acc = acc + shares[member][:, combo : combo + 1] * parts[
                member, combo * rows : (combo + 1) * rows, :
            ].astype(F32)
        sums.append(acc / total[:, combo : combo + 1])
    heads = []
    for head in range(2):
        attended = sums[2 * head] - lambdas[head] * sums[2 * head + 1]
        heads.append(rms(attended, head_gain[...]).astype(BF16))
    for copy in range(out.shape[0]):
        for head in range(2):
            out[copy, :rows, head * 128 : (head + 1) * 128] = heads[head]
        out[copy, rows:, :] = jnp.broadcast_to(dec_out[...], (out.shape[1] - rows, 256))


def combine(parts, dec_out, lambdas, head_gain, copies):
    rows = parts.shape[1] * 2 // 9
    return pl.pallas_call(
        combine_body,
        out_shape=jax.ShapeDtypeStruct((copies, rows + 8, 256), BF16),
        in_specs=vmem(2) + [pl.BlockSpec(memory_space=pltpu.SMEM)] + vmem(1),
        out_specs=vmem(1)[0],
        compiler_params=pltpu.CompilerParams(vmem_limit_bytes=16 * MIB),
        cost_estimate=pl.CostEstimate(flops=10**8, bytes_accessed=MIB, transcendentals=0),
        name="combine",
    )(parts, dec_out, lambdas, head_gain)


def out_body(heads, w, piece, dec):
    rows = piece.shape[0]
    acc = nn_dot(heads[0], w[:256])
    for copy in range(1, heads.shape[0]):
        acc = acc + nn_dot(heads[copy], w[copy * 256 : (copy + 1) * 256])
    piece[...] = acc[:rows].astype(BF16)
    dec[...] = acc[rows : rows + 1].astype(BF16)


def out_rows(heads, w, rows):
    return pl.pallas_call(
        out_body,
        out_shape=(
            jax.ShapeDtypeStruct((rows, w.shape[1]), BF16),
            jax.ShapeDtypeStruct((1, w.shape[1]), BF16),
        ),
        in_specs=vmem(2),
        out_specs=tuple(vmem(2)),
        compiler_params=pltpu.CompilerParams(vmem_limit_bytes=8 * MIB),
        cost_estimate=pl.CostEstimate(flops=10**8, bytes_accessed=MIB, transcendentals=0),
        name="out_rows",
    )(heads, w)


def layer(
    x_piece,
    x_decode,
    norm_gain,
    w_query,
    w_key,
    w_value,
    w_out,
    head_gain,
    lambdas,
    piece_keys,
    piece_values,
    cache_keys,
    cache_values,
    cache_lengths,
):
    kv_count = lax.axis_size("kv")
    tp_count = lax.axis_size("tp")
    members = kv_count // SHARE
    rows = x_piece.shape[0]
    groups = [
        [z * 8 + y * 2 + core for z in range(parity, 8, 2) for y in range(4)]
        for parity in range(2)
        for core in range(2)
    ]
    gain = norm_gain.reshape(1, -1)
    head_gain = head_gain.reshape(1, -1)
    me = lax.axis_index("kv")

    def across(i):
        z, y, core = i // 8, i // 2 % 4, i % 2
        z = z ^ 1 if core == 0 else (z + 2 * (z % 2) + 7) % 8
        return z * 8 + y * 2 + core

    ids = me.reshape(1)

    def move(array, target):
        return lax.ppermute(array, "kv", [(i, target(i)) for i in range(kv_count)])

    pool, sent, q_dec, row_dec = opening(
        piece_keys.reshape(-1, 128),
        piece_values.reshape(-1, 128),
        x_piece,
        x_decode,
        gain,
        w_query,
        members,
    )
    far = move(pool, across)
    pools = [pool, move(pool, lambda i: i ^ 1), far, move(far, lambda i: i ^ 1)]
    got = lax.all_to_all(sent, "kv", 0, 0, tiled=True, axis_index_groups=groups)
    k_new, v_new, k_dec, v_dec = fresh(row_dec, w_key, w_value, pools, rows)
    dec_out = decode(
        q_dec,
        k_dec,
        v_dec,
        cache_keys.reshape(-1, 128),
        cache_values.reshape(-1, 128),
        cache_lengths,
        lambdas,
        head_gain,
    )
    slots = piece_keys.shape[0]
    parts = attend(ids, got.reshape(members * rows, 256), pools, slots, k_new, v_new)
    parts = lax.all_to_all(
        parts, "kv", 0, 0, tiled=True, axis_index_groups=groups
    )
    heads = combine(parts, dec_out, lambdas, head_gain, tp_count)
    heads = lax.all_to_all(heads, "tp", 0, 0, tiled=True)
    return out_rows(heads, w_out, rows)


def solution(mesh):
    placed = (
        P("kv", None),
        P("kv", None),
        P(),
        P(None, "tp"),
        P(None, "tp"),
        P(None, "tp"),
        P(None, "tp"),
        P(),
        P("tp"),
        P("kv", "tp", None),
        P("kv", "tp", None),
        P("kv", None, "tp", None),
        P("kv", None, "tp", None),
        P("kv"),
    )
    return jax.shard_map(
        layer,
        mesh=mesh,
        in_specs=placed,
        out_specs=(P("kv", "tp"), P("kv", "tp")),
        check_vma=False,
    )
```

```python
import math

import jax
import jax.numpy as jnp
from jax import lax
from jax.experimental import pallas as pl
from jax.experimental.pallas import tpu as pltpu
from jax.sharding import PartitionSpec as P

EPS = 1e-06
SHARE = 4
NEG = -jnp.inf
F32 = jnp.float32
BF16 = jnp.bfloat16
MIB = 1024 * 1024
ATT, FRE, DEC, OPN = 20, 8, 52, 60


def nt_dot(a, b):
    return lax.dot_general(a, b, (((1,), (1,)), ((), ())), preferred_element_type=F32)


def nn_dot(a, b):
    return lax.dot_general(a, b, (((1,), (0,)), ((), ())), preferred_element_type=F32)


def lane_iota(shape):
    return lax.broadcasted_iota(jnp.int32, shape, len(shape) - 1)


def rms(rows, gain):
    return rows * lax.rsqrt(jnp.mean(rows * rows, axis=-1, keepdims=True) + EPS) * gain


def vmem(count):
    return [pl.BlockSpec(memory_space=pltpu.VMEM)] * count


HBM = pl.BlockSpec(memory_space=pltpu.HBM)


def fetch(pairs, sems):
    copies = [pltpu.make_async_copy(a, b, sems.at[i]) for i, (a, b) in enumerate(pairs)]
    for copy in copies:
        copy.start()
    return copies


def opening_body(
    keys, values, x, x_dec, gain, w, pool, out, out_dec, row_dec, kv, xs, xd, g, wq, wide, normed,
    sems
):

    copies = fetch(
        (
            (x, xs),
            (x_dec, xd),
            (gain, g),
            (w, wq),
            (keys, kv.at[0]),
            (values, kv.at[1]),
        ),
        sems,
    )
    slots = keys.shape[0] // 2
    rows = x.shape[0]
    for copy in copies[:3]:
        copy.wait()
    normed[:rows] = rms(xs[...].astype(F32), g[...]).astype(BF16)
    normed[rows:] = jnp.broadcast_to(
        rms(xd[...].astype(F32), g[...]).astype(BF16), (16, x.shape[1])
    )
    row_dec[...] = normed[rows : rows + 1]
    for tile in range(x.shape[1] // 128):
        at = slots + rows * (tile // 4)
        pool[tile % 4, at : at + rows, :] = normed[:rows, tile * 128 : (tile + 1) * 128]
    copies[3].wait()
    result = nn_dot(normed[...], wq[...]).astype(BF16)
    for member in range(out.shape[0]):
        out[member] = result[:rows]
    out_dec[...] = result[rows : rows + 1]
    for index in range(2):
        copies[4 + index].wait()
        wide[index] = kv[index].astype(F32)
        for head in range(2):
            pool[2 * head + index, :slots] = wide[index, pl.ds(head, slots, stride=2), :].astype(
                BF16
            )


def opening(keys, values, x, x_dec, gain, w, members):
    rows, width = x.shape
    slots = keys.shape[0] // 2
    return pl.pallas_call(
        opening_body,
        out_shape=(
            pltpu.VMEM((4, slots + rows * width // 512, 128), BF16),
            pltpu.VMEM((members, rows, w.shape[1]), BF16),
            jax.ShapeDtypeStruct((1, w.shape[1]), BF16),
            jax.ShapeDtypeStruct((1, width), BF16),
        ),
        in_specs=[HBM] * 6,
        out_specs=tuple(vmem(4)),
        scratch_shapes=[
            pltpu.VMEM((2, 2 * slots, 128), BF16),
            pltpu.VMEM((rows, width), BF16),
            pltpu.VMEM((1, width), BF16),
            pltpu.VMEM((1, width), F32),
            pltpu.VMEM(w.shape, BF16),
            pltpu.VMEM((2, 2 * slots, 128), F32),
            pltpu.VMEM((rows + 16, width), BF16),
            pltpu.SemaphoreType.DMA((6,)),
        ],
        compiler_params=pltpu.CompilerParams(vmem_limit_bytes=OPN * MIB),
        cost_estimate=pl.CostEstimate(flops=10**9, bytes_accessed=2 * MIB, transcendentals=0),
        name="opening",
    )(keys, values, x, x_dec, gain, w)


def decode_body(
    q_dec, k_dec, v_dec, keys, values, length, lambdas, head_gain, head_out, kc, vc, sems
):
    copies = fetch(((keys, kc), (values, vc)), sems)

    row = lax.broadcasted_iota(jnp.int32, (8, 128), 0)
    lane = lane_iota((8, 128))
    second = (row // 2) % 2 == 1

    def per_head(line):
        line = line.astype(F32)
        return jnp.where(
            second,
            jnp.broadcast_to(line[:, 128:], (8, 128)),
            jnp.broadcast_to(line[:, :128], (8, 128)),
        )

    half = lane // 64 == row % 2
    queries = jnp.where(half, per_head(q_dec[...]), 0.0)
    own_keys = per_head(k_dec[...])
    own_values = per_head(v_dec[...])
    scale = 0.125 * math.log2(math.e)
    copies[0].wait()
    scores = nt_dot(queries.astype(BF16), kc[...])
    width = keys.shape[0]
    column = lane_iota((8, width))
    wide_row = lax.broadcasted_iota(jnp.int32, (8, width), 0)
    allowed = (column % 2 == (wide_row // 2) % 2) & (column // 2 < length[0])
    scores = jnp.where(allowed, scores, NEG)
    own_score = jnp.sum(queries * own_keys, axis=-1, keepdims=True)
    row_max = jnp.maximum(jnp.max(scores, axis=-1, keepdims=True), own_score)
    weights = jnp.exp2((scores - row_max) * scale)
    own_weight = jnp.exp2((own_score - row_max) * scale)
    totals = jnp.sum(weights, axis=-1, keepdims=True) + own_weight
    copies[1].wait()
    mixed = nn_dot(weights.astype(BF16), vc[...])
    mixed = (mixed + own_weight.astype(BF16).astype(F32) * own_values) / totals
    for head in range(2):
        attended = mixed[2 * head : 2 * head + 1] - lambdas[head] * mixed[2 * head + 1 : 2 * head + 2]
        head_out[:, head * 128 : (head + 1) * 128] = rms(attended, head_gain[...]).astype(BF16)


def decode(q_dec, k_dec, v_dec, keys, values, length, lambdas, head_gain):
    smem = pl.BlockSpec(memory_space=pltpu.SMEM)
    return pl.pallas_call(
        decode_body,
        out_shape=pltpu.VMEM((1, 256), BF16),
        in_specs=vmem(3) + [HBM] * 2 + [smem, smem] + vmem(1),
        out_specs=vmem(1)[0],
        scratch_shapes=[
            pltpu.VMEM(keys.shape, BF16),
            pltpu.VMEM(values.shape, BF16),
            pltpu.SemaphoreType.DMA((2,)),
        ],
        compiler_params=pltpu.CompilerParams(vmem_limit_bytes=DEC * MIB),
        cost_estimate=pl.CostEstimate(flops=2 * 10**9, bytes_accessed=2 * MIB, transcendentals=0),
        name="decode",
    )(q_dec, k_dec, v_dec, keys, values, length, lambdas, head_gain)


def fresh_body(*refs):
    row_dec, w_key, w_value = refs[:3]
    pools = refs[3:7]
    k_out, v_out, k_dec, v_dec, xs, normed, sems = refs[7:]
    total = k_out.shape[0]
    rows = total // 4
    tiles = row_dec.shape[1] // 128
    slots = pools[0].shape[1] - rows * tiles // 4
    copies = fetch([(s.at[:, slots:], xs.at[i]) for i, s in enumerate(pools)], sems)
    normed[total:] = jnp.broadcast_to(row_dec[...], (16, row_dec.shape[1]))
    for index in range(4):
        copies[index].wait()
        for tile in range(tiles):
            normed[index * rows : (index + 1) * rows, tile * 128 : (tile + 1) * 128] = xs[
                index, tile % 4, rows * (tile // 4) : rows * (tile // 4 + 1), :
            ]
    for w, out, out_dec in ((w_key, k_out, k_dec), (w_value, v_out, v_dec)):
        result = nn_dot(normed[...], w[...]).astype(BF16)
        out[...] = result[:total]
        out_dec[...] = result[total : total + 1]


def fresh(row_dec, w_key, w_value, pools, rows):
    width = row_dec.shape[1]
    return pl.pallas_call(
        fresh_body,
        out_shape=(
            jax.ShapeDtypeStruct((4 * rows, 256), BF16),
            jax.ShapeDtypeStruct((4 * rows, 256), BF16),
            jax.ShapeDtypeStruct((1, 256), BF16),
            jax.ShapeDtypeStruct((1, 256), BF16),
        ),
        in_specs=vmem(3) + [HBM] * 4,
        out_specs=tuple(vmem(4)),
        scratch_shapes=[
            pltpu.VMEM((4, 4, rows * width // 512, 128), BF16),
            pltpu.VMEM((4 * rows + 16, width), BF16),
            pltpu.SemaphoreType.DMA((4,)),
        ],
        compiler_params=pltpu.CompilerParams(vmem_limit_bytes=FRE * MIB),
        cost_estimate=pl.CostEstimate(flops=10**9, bytes_accessed=2 * MIB, transcendentals=0),
        name="fresh",
    )(row_dec, w_key, w_value, *pools)


def attend_body(slots, *refs):
    ids, queries = refs[:2]
    sources = refs[2:6]
    k_new, v_new, out, pool, sems = refs[6:]
    copies = fetch(
        [
            (source.at[2 * head : 2 * head + 2, :slots], pool.at[i, 2 * head : 2 * head + 2])
            for head in range(2)
            for i, source in enumerate(sources)
        ],
        sems,
    )
    rows = queries.shape[0]
    fresh_rows = k_new.shape[0]
    each = fresh_rows // 4
    scale = 0.125 * math.log2(math.e)
    block = min(128, rows)
    me = ids[0]
    core = lax.rem(me, 2)
    y = lax.rem(lax.div(me, 2), 4)
    z = lax.div(me, 8)
    key_lane = lane_iota((block, fresh_rows))
    slot = key_lane // each
    of = jnp.bitwise_xor(core, slot % 2)
    z_of = jnp.where(of == 0, jnp.bitwise_xor(z, 1), lax.rem(z + 2 * lax.rem(z, 2) + 7, 8))
    owner = of + 2 * y + 8 * jnp.where(slot < 2, z, z_of)
    key_pos = each * owner + key_lane % each
    row = lax.broadcasted_iota(jnp.int32, (block, fresh_rows), 0)
    lane = lane_iota((block, 128))

    def score(task):
        head, which, start = task
        if which == 0 and start == 0:
            for copy in copies[4 * head : 4 * head + 4]:
                copy.wait()
        cols = slice(head * 128, (head + 1) * 128)
        q = queries[start : start + block, cols].astype(F32)
        kept = (lane < 64) if which == 0 else (lane >= 64)
        masked = jnp.where(kept, q, 0.0).astype(BF16)
        at = row + start
        member = at // each
        place = 8 * (2 * (member // 4) + lax.rem(z, 2)) + 2 * (member % 4) + core
        row_pos = each * place + at % each
        last = jnp.where(key_pos <= row_pos, nt_dot(masked, k_new[:, cols]), NEG)
        return [nt_dot(masked, pool[i, 2 * head]) for i in range(4)], last

    stats = {start: jnp.zeros((block, 128), F32) for start in range(0, rows, block)}

    def finish(task, scores, last):
        head, which, start = task
        combo = 2 * head + which
        row_max = jnp.max(last, axis=-1, keepdims=True)
        for s in scores:
            row_max = jnp.maximum(row_max, jnp.max(s, axis=-1, keepdims=True))
        weights = jnp.exp2((last - row_max) * scale)
        total = jnp.sum(weights, axis=-1, keepdims=True)
        mixed = nn_dot(weights.astype(BF16), v_new[:, head * 128 : (head + 1) * 128])
        for i, s in enumerate(scores):
            weights = jnp.exp2((s - row_max) * scale)
            total = total + jnp.sum(weights, axis=-1, keepdims=True)
            mixed = mixed + nn_dot(weights.astype(BF16), pool[i, 2 * head + 1])
        mixed = mixed / total
        place = slice(start // each, (start + block) // each)
        out[place, combo * each : (combo + 1) * each, :] = mixed.astype(BF16).reshape(
            block // each, each, 128
        )
        for base, stat in ((0, row_max), (4, total)):
            for part in range(3):
                piece = stat.astype(BF16).astype(F32)
                at = lane % 64 == 8 * part + base + combo
                stats[start] = jnp.where(at, piece, stats[start])
                stat = stat - piece

    tasks = [(h, w, start) for h in range(2) for w in range(2) for start in range(0, rows, block)]
    ahead = score(tasks[0])
    for index, task in enumerate(tasks):
        ready = ahead
        if index + 1 < len(tasks):
            ahead = score(tasks[index + 1])
        finish(task, *ready)
    low = lane_iota((block // each, each // 2, 128)) < 64
    for start in range(0, rows, block):
        pair = stats[start].reshape(block // each, 2, each // 2, 128)
        place = slice(start // each, (start + block) // each)
        out[place, 4 * each :, :] = jnp.where(low, pair[:, 0], pair[:, 1]).astype(BF16)


def attend(ids, queries, pools, slots, k_new, v_new):
    rows = queries.shape[0]
    keys = 4 * slots + k_new.shape[0]
    each = k_new.shape[0] // 4
    return pl.pallas_call(
        lambda *refs: attend_body(slots, *refs),
        out_shape=pltpu.HBM((rows // each, 4 * each + each // 2, 128), BF16),
        in_specs=[pl.BlockSpec(memory_space=pltpu.SMEM)] + vmem(1) + [HBM] * 4 + vmem(2),
        out_specs=vmem(1)[0],
        scratch_shapes=[
            pltpu.VMEM((4, 4, slots, 128), BF16),
            pltpu.SemaphoreType.DMA((8,)),
        ],
        compiler_params=pltpu.CompilerParams(vmem_limit_bytes=ATT * MIB),
        cost_estimate=pl.CostEstimate(
            flops=4 * rows * keys * 512, bytes_accessed=2 * MIB, transcendentals=4 * rows * keys
        ),
        name="attend",
    )(ids, queries, *pools, k_new, v_new)


def combine_body(parts, dec_out, lambdas, head_gain, out):
    scale = 0.125 * math.log2(math.e)
    members = parts.shape[0]
    rows = parts.shape[1] * 2 // 9

    def whole(member):
        pieces = parts[member, 4 * rows :, :].astype(F32)
        pieces = jnp.concatenate([pieces, pltpu.roll(pieces, 64, 1)], axis=0)
        return pieces + pltpu.roll(pieces, 120, 1) + pltpu.roll(pieces, 112, 1)

    stats = [whole(member) for member in range(members)]
    top = stats[0]
    for s in stats[1:]:
        top = jnp.maximum(top, s)
    shares = [jnp.exp2((s - top) * scale) * pltpu.roll(s, 124, 1) for s in stats]
    total = shares[0]
    for s in shares[1:]:
        total = total + s
    sums = []
    for combo in range(4):
        acc = jnp.zeros((rows, 128), F32)
        for member in range(members):
            acc = acc + shares[member][:, combo : combo + 1] * parts[
                member, combo * rows : (combo + 1) * rows, :
            ].astype(F32)
        sums.append(acc / total[:, combo : combo + 1])
    heads = []
    for head in range(2):
        attended = sums[2 * head] - lambdas[head] * sums[2 * head + 1]
        heads.append(rms(attended, head_gain[...]).astype(BF16))
    for copy in range(out.shape[0]):
        for head in range(2):
            out[copy, :rows, head * 128 : (head + 1) * 128] = heads[head]
        out[copy, rows:, :] = jnp.broadcast_to(dec_out[...], (out.shape[1] - rows, 256))


def combine(parts, dec_out, lambdas, head_gain, copies):
    rows = parts.shape[1] * 2 // 9
    return pl.pallas_call(
        combine_body,
        out_shape=jax.ShapeDtypeStruct((copies, rows + 8, 256), BF16),
        in_specs=vmem(2) + [pl.BlockSpec(memory_space=pltpu.SMEM)] + vmem(1),
        out_specs=vmem(1)[0],
        compiler_params=pltpu.CompilerParams(vmem_limit_bytes=16 * MIB),
        cost_estimate=pl.CostEstimate(flops=10**8, bytes_accessed=MIB, transcendentals=0),
        name="combine",
    )(parts, dec_out, lambdas, head_gain)


def out_body(heads, w, piece, dec):
    rows = piece.shape[0]
    acc = nn_dot(heads[0], w[:256])
    for copy in range(1, heads.shape[0]):
        acc = acc + nn_dot(heads[copy], w[copy * 256 : (copy + 1) * 256])
    piece[...] = acc[:rows].astype(BF16)
    dec[...] = acc[rows : rows + 1].astype(BF16)


def out_rows(heads, w, rows):
    return pl.pallas_call(
        out_body,
        out_shape=(
            jax.ShapeDtypeStruct((rows, w.shape[1]), BF16),
            jax.ShapeDtypeStruct((1, w.shape[1]), BF16),
        ),
        in_specs=vmem(2),
        out_specs=tuple(vmem(2)),
        compiler_params=pltpu.CompilerParams(vmem_limit_bytes=8 * MIB),
        cost_estimate=pl.CostEstimate(flops=10**8, bytes_accessed=MIB, transcendentals=0),
        name="out_rows",
    )(heads, w)


def layer(
    x_piece,
    x_decode,
    norm_gain,
    w_query,
    w_key,
    w_value,
    w_out,
    head_gain,
    lambdas,
    piece_keys,
    piece_values,
    cache_keys,
    cache_values,
    cache_lengths,
):
    kv_count = lax.axis_size("kv")
    tp_count = lax.axis_size("tp")
    members = kv_count // SHARE
    rows = x_piece.shape[0]
    groups = [
        [z * 8 + y * 2 + core for z in range(parity, 8, 2) for y in range(4)]
        for parity in range(2)
        for core in range(2)
    ]
    gain = norm_gain.reshape(1, -1)
    head_gain = head_gain.reshape(1, -1)
    me = lax.axis_index("kv")

    def across(i):
        z, y, core = i // 8, i // 2 % 4, i % 2
        z = z ^ 1 if core == 0 else (z + 2 * (z % 2) + 7) % 8
        return z * 8 + y * 2 + core

    ids = me.reshape(1)

    def move(array, target):
        return lax.ppermute(array, "kv", [(i, target(i)) for i in range(kv_count)])

    pool, sent, q_dec, row_dec = opening(
        piece_keys.reshape(-1, 128),
        piece_values.reshape(-1, 128),
        x_piece,
        x_decode,
        gain,
        w_query,
        members,
    )
    far = move(pool, across)
    pools = [pool, move(pool, lambda i: i ^ 1), far, move(far, lambda i: i ^ 1)]
    got = lax.all_to_all(sent, "kv", 0, 0, tiled=True, axis_index_groups=groups)
    k_new, v_new, k_dec, v_dec = fresh(row_dec, w_key, w_value, pools, rows)
    dec_out = decode(
        q_dec,
        k_dec,
        v_dec,
        cache_keys.reshape(-1, 128),
        cache_values.reshape(-1, 128),
        cache_lengths,
        lambdas,
        head_gain,
    )
    slots = piece_keys.shape[0]
    parts = attend(ids, got.reshape(members * rows, 256), pools, slots, k_new, v_new)
    parts = lax.all_to_all(
        parts, "kv", 0, 0, tiled=True, axis_index_groups=groups
    )
    heads = combine(parts, dec_out, lambdas, head_gain, tp_count)
    heads = lax.all_to_all(heads, "tp", 0, 0, tiled=True)
    return out_rows(heads, w_out, rows)


def solution(mesh):
    placed = (
        P("kv", None),
        P("kv", None),
        P(),
        P(None, "tp"),
        P(None, "tp"),
        P(None, "tp"),
        P(None, "tp"),
        P(),
        P("tp"),
        P("kv", "tp", None),
        P("kv", "tp", None),
        P("kv", None, "tp", None),
        P("kv", None, "tp", None),
        P("kv"),
    )
    return jax.shard_map(
        layer,
        mesh=mesh,
        in_specs=placed,
        out_specs=(P("kv", "tp"), P("kv", "tp")),
        check_vma=False,
    )
```

```python
import math

import jax
import jax.numpy as jnp
from jax import lax
from jax.experimental import pallas as pl
from jax.experimental.pallas import tpu as pltpu
from jax.sharding import PartitionSpec as P

EPS = 1e-06
SHARE = 4
NEG = -jnp.inf
F32 = jnp.float32
BF16 = jnp.bfloat16
MIB = 1024 * 1024
ATT, FRE, DEC, OPN = 20, 8, 52, 60


def nt_dot(a, b):
    return lax.dot_general(a, b, (((1,), (1,)), ((), ())), preferred_element_type=F32)


def nn_dot(a, b):
    return lax.dot_general(a, b, (((1,), (0,)), ((), ())), preferred_element_type=F32)


def lane_iota(shape):
    return lax.broadcasted_iota(jnp.int32, shape, len(shape) - 1)


def rms(rows, gain):
    return rows * lax.rsqrt(jnp.mean(rows * rows, axis=-1, keepdims=True) + EPS) * gain


def vmem(count):
    return [pl.BlockSpec(memory_space=pltpu.VMEM)] * count


HBM = pl.BlockSpec(memory_space=pltpu.HBM)


def fetch(pairs, sems):
    copies = [pltpu.make_async_copy(a, b, sems.at[i]) for i, (a, b) in enumerate(pairs)]
    for copy in copies:
        copy.start()
    return copies


def opening_body(
    keys, values, x, x_dec, gain, w, pool, out_hbm, out_dec, row_dec, kv, xs, xd, g, wq, wide, normed,
    out, sems
):

    copies = fetch(
        (
            (x, xs),
            (x_dec, xd),
            (gain, g),
            (w, wq),
            (keys, kv.at[0]),
            (values, kv.at[1]),
        ),
        sems,
    )
    slots = keys.shape[0] // 2
    rows = x.shape[0]
    for copy in copies[:3]:
        copy.wait()
    normed[:rows] = rms(xs[...].astype(F32), g[...]).astype(BF16)
    normed[rows:] = jnp.broadcast_to(
        rms(xd[...].astype(F32), g[...]).astype(BF16), (16, x.shape[1])
    )
    row_dec[...] = normed[rows : rows + 1]
    for tile in range(x.shape[1] // 128):
        at = slots + rows * (tile // 4)
        pool[tile % 4, at : at + rows, :] = normed[:rows, tile * 128 : (tile + 1) * 128]
    copies[3].wait()
    result = nn_dot(normed[...], wq[...]).astype(BF16)
    for member in range(out.shape[0]):
        out[member] = result[:rows]
    out_dec[...] = result[rows : rows + 1]
    sent = pltpu.make_async_copy(out, out_hbm, sems.at[6])
    sent.start()
    for index in range(2):
        copies[4 + index].wait()
        wide[index] = kv[index].astype(F32)
        for head in range(2):
            pool[2 * head + index, :slots] = wide[index, pl.ds(head, slots, stride=2), :].astype(
                BF16
            )
    sent.wait()


def opening(keys, values, x, x_dec, gain, w, members):
    rows, width = x.shape
    slots = keys.shape[0] // 2
    return pl.pallas_call(
        opening_body,
        out_shape=(
            pltpu.VMEM((4, slots + rows * width // 512, 128), BF16),
            pltpu.HBM((members, rows, w.shape[1]), BF16),
            jax.ShapeDtypeStruct((1, w.shape[1]), BF16),
            jax.ShapeDtypeStruct((1, width), BF16),
        ),
        in_specs=[HBM] * 6,
        out_specs=(vmem(1)[0], HBM, *vmem(2)),
        scratch_shapes=[
            pltpu.VMEM((2, 2 * slots, 128), BF16),
            pltpu.VMEM((rows, width), BF16),
            pltpu.VMEM((1, width), BF16),
            pltpu.VMEM((1, width), F32),
            pltpu.VMEM(w.shape, BF16),
            pltpu.VMEM((2, 2 * slots, 128), F32),
            pltpu.VMEM((rows + 16, width), BF16),
            pltpu.VMEM((members, rows, w.shape[1]), BF16),
            pltpu.SemaphoreType.DMA((7,)),
        ],
        compiler_params=pltpu.CompilerParams(vmem_limit_bytes=OPN * MIB),
        cost_estimate=pl.CostEstimate(flops=10**9, bytes_accessed=2 * MIB, transcendentals=0),
        name="opening",
    )(keys, values, x, x_dec, gain, w)


def decode_body(
    q_dec, k_dec, v_dec, keys, values, length, lambdas, head_gain, head_out, kc, vc, sems
):
    copies = fetch(((keys, kc), (values, vc)), sems)

    row = lax.broadcasted_iota(jnp.int32, (8, 128), 0)
    lane = lane_iota((8, 128))
    second = (row // 2) % 2 == 1

    def per_head(line):
        line = line.astype(F32)
        return jnp.where(
            second,
            jnp.broadcast_to(line[:, 128:], (8, 128)),
            jnp.broadcast_to(line[:, :128], (8, 128)),
        )

    half = lane // 64 == row % 2
    queries = jnp.where(half, per_head(q_dec[...]), 0.0)
    own_keys = per_head(k_dec[...])
    own_values = per_head(v_dec[...])
    scale = 0.125 * math.log2(math.e)
    copies[0].wait()
    scores = nt_dot(queries.astype(BF16), kc[...])
    width = keys.shape[0]
    column = lane_iota((8, width))
    wide_row = lax.broadcasted_iota(jnp.int32, (8, width), 0)
    allowed = (column % 2 == (wide_row // 2) % 2) & (column // 2 < length[0])
    scores = jnp.where(allowed, scores, NEG)
    own_score = jnp.sum(queries * own_keys, axis=-1, keepdims=True)
    row_max = jnp.maximum(jnp.max(scores, axis=-1, keepdims=True), own_score)
    weights = jnp.exp2((scores - row_max) * scale)
    own_weight = jnp.exp2((own_score - row_max) * scale)
    totals = jnp.sum(weights, axis=-1, keepdims=True) + own_weight
    copies[1].wait()
    mixed = nn_dot(weights.astype(BF16), vc[...])
    mixed = (mixed + own_weight.astype(BF16).astype(F32) * own_values) / totals
    for head in range(2):
        attended = mixed[2 * head : 2 * head + 1] - lambdas[head] * mixed[2 * head + 1 : 2 * head + 2]
        head_out[:, head * 128 : (head + 1) * 128] = rms(attended, head_gain[...]).astype(BF16)


def decode(q_dec, k_dec, v_dec, keys, values, length, lambdas, head_gain):
    smem = pl.BlockSpec(memory_space=pltpu.SMEM)
    return pl.pallas_call(
        decode_body,
        out_shape=pltpu.VMEM((1, 256), BF16),
        in_specs=vmem(3) + [HBM] * 2 + [smem, smem] + vmem(1),
        out_specs=vmem(1)[0],
        scratch_shapes=[
            pltpu.VMEM(keys.shape, BF16),
            pltpu.VMEM(values.shape, BF16),
            pltpu.SemaphoreType.DMA((2,)),
        ],
        compiler_params=pltpu.CompilerParams(vmem_limit_bytes=DEC * MIB),
        cost_estimate=pl.CostEstimate(flops=2 * 10**9, bytes_accessed=2 * MIB, transcendentals=0),
        name="decode",
    )(q_dec, k_dec, v_dec, keys, values, length, lambdas, head_gain)


def fresh_body(*refs):
    row_dec, w_key, w_value = refs[:3]
    pools = refs[3:7]
    k_out, v_out, k_dec, v_dec, xs, normed, sems = refs[7:]
    total = k_out.shape[0]
    rows = total // 4
    tiles = row_dec.shape[1] // 128
    slots = pools[0].shape[1] - rows * tiles // 4
    copies = fetch([(s.at[:, slots:], xs.at[i]) for i, s in enumerate(pools)], sems)
    normed[total:] = jnp.broadcast_to(row_dec[...], (16, row_dec.shape[1]))
    for index in range(4):
        copies[index].wait()
        for tile in range(tiles):
            normed[index * rows : (index + 1) * rows, tile * 128 : (tile + 1) * 128] = xs[
                index, tile % 4, rows * (tile // 4) : rows * (tile // 4 + 1), :
            ]
    for w, out, out_dec in ((w_key, k_out, k_dec), (w_value, v_out, v_dec)):
        result = nn_dot(normed[...], w[...]).astype(BF16)
        out[...] = result[:total]
        out_dec[...] = result[total : total + 1]


def fresh(row_dec, w_key, w_value, pools, rows):
    width = row_dec.shape[1]
    return pl.pallas_call(
        fresh_body,
        out_shape=(
            jax.ShapeDtypeStruct((4 * rows, 256), BF16),
            jax.ShapeDtypeStruct((4 * rows, 256), BF16),
            jax.ShapeDtypeStruct((1, 256), BF16),
            jax.ShapeDtypeStruct((1, 256), BF16),
        ),
        in_specs=vmem(3) + [HBM] * 4,
        out_specs=tuple(vmem(4)),
        scratch_shapes=[
            pltpu.VMEM((4, 4, rows * width // 512, 128), BF16),
            pltpu.VMEM((4 * rows + 16, width), BF16),
            pltpu.SemaphoreType.DMA((4,)),
        ],
        compiler_params=pltpu.CompilerParams(vmem_limit_bytes=FRE * MIB),
        cost_estimate=pl.CostEstimate(flops=10**9, bytes_accessed=2 * MIB, transcendentals=0),
        name="fresh",
    )(row_dec, w_key, w_value, *pools)


def attend_body(slots, *refs):
    ids, queries = refs[:2]
    sources = refs[2:6]
    k_new, v_new, out, pool, sems = refs[6:]
    copies = fetch(
        [
            (source.at[2 * head : 2 * head + 2, :slots], pool.at[i, 2 * head : 2 * head + 2])
            for head in range(2)
            for i, source in enumerate(sources)
        ],
        sems,
    )
    rows = queries.shape[0]
    fresh_rows = k_new.shape[0]
    each = fresh_rows // 4
    scale = 0.125 * math.log2(math.e)
    block = min(128, rows)
    me = ids[0]
    core = lax.rem(me, 2)
    y = lax.rem(lax.div(me, 2), 4)
    z = lax.div(me, 8)
    key_lane = lane_iota((block, fresh_rows))
    slot = key_lane // each
    of = jnp.bitwise_xor(core, slot % 2)
    z_of = jnp.where(of == 0, jnp.bitwise_xor(z, 1), lax.rem(z + 2 * lax.rem(z, 2) + 7, 8))
    owner = of + 2 * y + 8 * jnp.where(slot < 2, z, z_of)
    key_pos = each * owner + key_lane % each
    row = lax.broadcasted_iota(jnp.int32, (block, fresh_rows), 0)
    lane = lane_iota((block, 128))

    def score(task):
        head, which, start = task
        if which == 0 and start == 0:
            for copy in copies[4 * head : 4 * head + 4]:
                copy.wait()
        cols = slice(head * 128, (head + 1) * 128)
        q = queries[start : start + block, cols].astype(F32)
        kept = (lane < 64) if which == 0 else (lane >= 64)
        masked = jnp.where(kept, q, 0.0).astype(BF16)
        at = row + start
        member = at // each
        place = 8 * (2 * (member // 4) + lax.rem(z, 2)) + 2 * (member % 4) + core
        row_pos = each * place + at % each
        last = jnp.where(key_pos <= row_pos, nt_dot(masked, k_new[:, cols]), NEG)
        return [nt_dot(masked, pool[i, 2 * head]) for i in range(4)], last

    stats = {start: jnp.zeros((block, 128), F32) for start in range(0, rows, block)}

    def finish(task, scores, last):
        head, which, start = task
        combo = 2 * head + which
        row_max = jnp.max(last, axis=-1, keepdims=True)
        for s in scores:
            row_max = jnp.maximum(row_max, jnp.max(s, axis=-1, keepdims=True))
        weights = jnp.exp2((last - row_max) * scale)
        total = jnp.sum(weights, axis=-1, keepdims=True)
        mixed = nn_dot(weights.astype(BF16), v_new[:, head * 128 : (head + 1) * 128])
        for i, s in enumerate(scores):
            weights = jnp.exp2((s - row_max) * scale)
            total = total + jnp.sum(weights, axis=-1, keepdims=True)
            mixed = mixed + nn_dot(weights.astype(BF16), pool[i, 2 * head + 1])
        mixed = mixed / total
        place = slice(start // each, (start + block) // each)
        out[place, combo * each : (combo + 1) * each, :] = mixed.astype(BF16).reshape(
            block // each, each, 128
        )
        for base, stat in ((0, row_max), (4, total)):
            for part in range(3):
                piece = stat.astype(BF16).astype(F32)
                at = lane % 64 == 8 * part + base + combo
                stats[start] = jnp.where(at, piece, stats[start])
                stat = stat - piece

    tasks = [(h, w, start) for h in range(2) for w in range(2) for start in range(0, rows, block)]
    ahead = score(tasks[0])
    for index, task in enumerate(tasks):
        ready = ahead
        if index + 1 < len(tasks):
            ahead = score(tasks[index + 1])
        finish(task, *ready)
    low = lane_iota((block // each, each // 2, 128)) < 64
    for start in range(0, rows, block):
        pair = stats[start].reshape(block // each, 2, each // 2, 128)
        place = slice(start // each, (start + block) // each)
        out[place, 4 * each :, :] = jnp.where(low, pair[:, 0], pair[:, 1]).astype(BF16)


def attend(ids, queries, pools, slots, k_new, v_new):
    rows = queries.shape[0]
    keys = 4 * slots + k_new.shape[0]
    each = k_new.shape[0] // 4
    return pl.pallas_call(
        lambda *refs: attend_body(slots, *refs),
        out_shape=pltpu.HBM((rows // each, 4 * each + each // 2, 128), BF16),
        in_specs=[pl.BlockSpec(memory_space=pltpu.SMEM)] + vmem(1) + [HBM] * 4 + vmem(2),
        out_specs=vmem(1)[0],
        scratch_shapes=[
            pltpu.VMEM((4, 4, slots, 128), BF16),
            pltpu.SemaphoreType.DMA((8,)),
        ],
        compiler_params=pltpu.CompilerParams(vmem_limit_bytes=ATT * MIB),
        cost_estimate=pl.CostEstimate(
            flops=4 * rows * keys * 512, bytes_accessed=2 * MIB, transcendentals=4 * rows * keys
        ),
        name="attend",
    )(ids, queries, *pools, k_new, v_new)


def combine_body(parts, dec_out, lambdas, head_gain, out):
    scale = 0.125 * math.log2(math.e)
    members = parts.shape[0]
    rows = parts.shape[1] * 2 // 9

    def whole(member):
        pieces = parts[member, 4 * rows :, :].astype(F32)
        pieces = jnp.concatenate([pieces, pltpu.roll(pieces, 64, 1)], axis=0)
        return pieces + pltpu.roll(pieces, 120, 1) + pltpu.roll(pieces, 112, 1)

    stats = [whole(member) for member in range(members)]
    top = stats[0]
    for s in stats[1:]:
        top = jnp.maximum(top, s)
    shares = [jnp.exp2((s - top) * scale) * pltpu.roll(s, 124, 1) for s in stats]
    total = shares[0]
    for s in shares[1:]:
        total = total + s
    sums = []
    for combo in range(4):
        acc = jnp.zeros((rows, 128), F32)
        for member in range(members):
            acc = acc + shares[member][:, combo : combo + 1] * parts[
                member, combo * rows : (combo + 1) * rows, :
            ].astype(F32)
        sums.append(acc / total[:, combo : combo + 1])
    heads = []
    for head in range(2):
        attended = sums[2 * head] - lambdas[head] * sums[2 * head + 1]
        heads.append(rms(attended, head_gain[...]).astype(BF16))
    for copy in range(out.shape[0]):
        for head in range(2):
            out[copy, :rows, head * 128 : (head + 1) * 128] = heads[head]
        out[copy, rows:, :] = jnp.broadcast_to(dec_out[...], (out.shape[1] - rows, 256))


def combine(parts, dec_out, lambdas, head_gain, copies):
    rows = parts.shape[1] * 2 // 9
    return pl.pallas_call(
        combine_body,
        out_shape=jax.ShapeDtypeStruct((copies, rows + 8, 256), BF16),
        in_specs=vmem(2) + [pl.BlockSpec(memory_space=pltpu.SMEM)] + vmem(1),
        out_specs=vmem(1)[0],
        compiler_params=pltpu.CompilerParams(vmem_limit_bytes=16 * MIB),
        cost_estimate=pl.CostEstimate(flops=10**8, bytes_accessed=MIB, transcendentals=0),
        name="combine",
    )(parts, dec_out, lambdas, head_gain)


def out_body(heads, w, piece, dec):
    rows = piece.shape[0]
    acc = nn_dot(heads[0], w[:256])
    for copy in range(1, heads.shape[0]):
        acc = acc + nn_dot(heads[copy], w[copy * 256 : (copy + 1) * 256])
    piece[...] = acc[:rows].astype(BF16)
    dec[...] = acc[rows : rows + 1].astype(BF16)


def out_rows(heads, w, rows):
    return pl.pallas_call(
        out_body,
        out_shape=(
            jax.ShapeDtypeStruct((rows, w.shape[1]), BF16),
            jax.ShapeDtypeStruct((1, w.shape[1]), BF16),
        ),
        in_specs=vmem(2),
        out_specs=tuple(vmem(2)),
        compiler_params=pltpu.CompilerParams(vmem_limit_bytes=8 * MIB),
        cost_estimate=pl.CostEstimate(flops=10**8, bytes_accessed=MIB, transcendentals=0),
        name="out_rows",
    )(heads, w)


def layer(
    x_piece,
    x_decode,
    norm_gain,
    w_query,
    w_key,
    w_value,
    w_out,
    head_gain,
    lambdas,
    piece_keys,
    piece_values,
    cache_keys,
    cache_values,
    cache_lengths,
):
    kv_count = lax.axis_size("kv")
    tp_count = lax.axis_size("tp")
    members = kv_count // SHARE
    rows = x_piece.shape[0]
    groups = [
        [z * 8 + y * 2 + core for z in range(parity, 8, 2) for y in range(4)]
        for parity in range(2)
        for core in range(2)
    ]
    gain = norm_gain.reshape(1, -1)
    head_gain = head_gain.reshape(1, -1)
    me = lax.axis_index("kv")

    def across(i):
        z, y, core = i // 8, i // 2 % 4, i % 2
        z = z ^ 1 if core == 0 else (z + 2 * (z % 2) + 7) % 8
        return z * 8 + y * 2 + core

    ids = me.reshape(1)

    def move(array, target):
        return lax.ppermute(array, "kv", [(i, target(i)) for i in range(kv_count)])

    pool, sent, q_dec, row_dec = opening(
        piece_keys.reshape(-1, 128),
        piece_values.reshape(-1, 128),
        x_piece,
        x_decode,
        gain,
        w_query,
        members,
    )
    far = move(pool, across)
    pools = [pool, move(pool, lambda i: i ^ 1), far, move(far, lambda i: i ^ 1)]
    got = lax.all_to_all(sent, "kv", 0, 0, tiled=True, axis_index_groups=groups)
    k_new, v_new, k_dec, v_dec = fresh(row_dec, w_key, w_value, pools, rows)
    dec_out = decode(
        q_dec,
        k_dec,
        v_dec,
        cache_keys.reshape(-1, 128),
        cache_values.reshape(-1, 128),
        cache_lengths,
        lambdas,
        head_gain,
    )
    slots = piece_keys.shape[0]
    parts = attend(ids, got.reshape(members * rows, 256), pools, slots, k_new, v_new)
    parts = lax.all_to_all(
        parts, "kv", 0, 0, tiled=True, axis_index_groups=groups
    )
    heads = combine(parts, dec_out, lambdas, head_gain, tp_count)
    heads = lax.all_to_all(heads, "tp", 0, 0, tiled=True)
    return out_rows(heads, w_out, rows)


def solution(mesh):
    placed = (
        P("kv", None),
        P("kv", None),
        P(),
        P(None, "tp"),
        P(None, "tp"),
        P(None, "tp"),
        P(None, "tp"),
        P(),
        P("tp"),
        P("kv", "tp", None),
        P("kv", "tp", None),
        P("kv", None, "tp", None),
        P("kv", None, "tp", None),
        P("kv"),
    )
    return jax.shard_map(
        layer,
        mesh=mesh,
        in_specs=placed,
        out_specs=(P("kv", "tp"), P("kv", "tp")),
        check_vma=False,
    )
```
